256 devices in a mesh: sp: 64 (over z, y, core), tp: 4 (over x).
Axes of the slice: x: 4, y: 4, z: 8, core: 2. Of those that a mesh axis runs over, the one named last changes fastest.
Arguments:
- stream: bfloat16 [16384, 2048], P(('sp', 'tp')), may hold values from -6 to 6
- query_one: bfloat16 [16384, 512], P('sp', 'tp'), may hold values from -280 to 280
- key_one: bfloat16 [16384, 512], P('sp', 'tp'), may hold values from -6 to 6
- query_two: bfloat16 [16384, 512], P('sp', 'tp'), may hold values from -280 to 280
- key_two: bfloat16 [16384, 512], P('sp', 'tp'), may hold values from -6 to 6
- values: bfloat16 [16384, 1024], P('sp', 'tp'), may hold values from -6 to 6
- lambdas: float32 [8], P('tp'), may hold values from 0.3 to 0.8
- head_gain: float32 [128], replicated, may hold values from 0.1 to 1.9
- out_weight: bfloat16 [1024, 2048], replicated, may hold values from -0.1875 to 0.1875
- norm_gain: float32 [2048], replicated, may hold values from 0.1 to 1.9
- gate_weight: bfloat16 [2048, 2816], P('sp', 'tp'), may hold values from -0.125 to 0.125
- up_weight: bfloat16 [2048, 2816], P('sp', 'tp'), may hold values from -0.125 to 0.125
- down_weight: bfloat16 [2816, 2048], P('tp', 'sp'), may hold values from -0.3125 to 0.3125
Outputs:
- result: bfloat16 [16384, 2048], P(('sp', 'tp'))
The draws below stay inside these ranges and needn't reach their ends.
All inputs are finite; a program needn't handle non-finite values.
Results may differ from the reference program's by a relative error of at most 0.014.
Values may be sent and summed in bfloat16 or wider, within the bound.
A program may use at most 128 MiB of HBM per device.

```python
import jax
import jax.numpy as jnp
from jax import lax

D = 2048
HEADS = 8
HEAD_DIM = 64
VDIM = 128
FF = 2816
SEQ = 16384
N_TP = 4


def drawn_pair(key, tag):
    folded = jax.random.fold_in(key, tag)
    query_seed, key_seed = jax.random.split(folded)
    row_width = HEADS * HEAD_DIM
    queries = jnp.clip(jax.random.normal(query_seed, (SEQ, row_width), jnp.float32), -6.0, 6.0) * 1.75
    keys = jnp.clip(jax.random.normal(key_seed, (SEQ, row_width), jnp.float32), -6.0, 6.0)
    return (queries, keys)


def draw_query_one(key, part):
    return drawn_pair(key, 11)[0].astype(jnp.bfloat16)


def draw_key_one(key, part):
    return drawn_pair(key, 11)[1].astype(jnp.bfloat16)


def draw_query_two(key, part):
    return drawn_pair(key, 23)[0].astype(jnp.bfloat16)


def draw_key_two(key, part):
    return drawn_pair(key, 23)[1].astype(jnp.bfloat16)


def block_scale(key, extent, pieces, least, largest):
    factor_of, own = 1.0, jax.random.fold_in(key, 6)
    for axis_at, blocks in pieces:
        steps = jnp.exp(jax.random.uniform(jax.random.fold_in(own, axis_at), (blocks,), jnp.float32, least / len(pieces), largest / len(pieces)))
        factor_of = factor_of * jnp.repeat(steps, extent[axis_at] // blocks).reshape([-1 if axis == axis_at else 1 for axis in range(len(extent))])
    return factor_of


def noise(key, extent, width, bound, cuts=(), kind=jnp.bfloat16):
    values = width * jax.random.normal(key, extent, jnp.float32)
    if cuts:
        values = values * block_scale(key, extent, cuts, -0.22, 0.18)
    return jnp.clip(values, -bound, bound).astype(kind)


def setup_inputs(seed: int = 0) -> dict:
    key_of = jax.random.split(jax.random.key(seed), 14)
    return {
        "stream": noise(key_of[0], (SEQ, D), 1.0, 6.0, ((0, 256),)),
        "query_one": draw_query_one(jax.random.fold_in(key_of[13], 71), 0),
        "key_one": draw_key_one(jax.random.fold_in(key_of[13], 71), 0),
        "query_two": draw_query_two(jax.random.fold_in(key_of[13], 71), 0),
        "key_two": draw_key_two(jax.random.fold_in(key_of[13], 71), 0),
        "values": noise(key_of[5], (SEQ, HEADS * VDIM), 1.0, 6.0, ((0, 64), (1, 4))),
        "lambdas": jnp.clip(0.3 + 0.5 * jax.random.uniform(key_of[6], (HEADS,), jnp.float32) ** block_scale(key_of[6], (HEADS,), ((0, 4),), -0.2, 0.2), 0.3, 0.8),
        "head_gain": jnp.clip(1.0 + 0.18 * jax.random.normal(key_of[7], (VDIM,), jnp.float32), 0.1, 1.9),
        "out_weight": noise(key_of[8], (HEADS * VDIM, D), (HEADS * VDIM) ** -0.5, 0.1875),
        "norm_gain": jnp.clip(1.0 + 0.18 * jax.random.normal(key_of[9], (D,), jnp.float32), 0.1, 1.9),
        "gate_weight": noise(key_of[10], (D, FF), D ** -0.5, 0.125, ((0, 64), (1, 4))),
        "up_weight": noise(key_of[11], (D, FF), D ** -0.5, 0.125, ((0, 64), (1, 4))),
        "down_weight": noise(key_of[12], (FF, D), (FF // 9) ** -0.5, 0.3125, ((0, 4), (1, 64))),
    }


ALPHA = 1.4142135623730951
EPSILON = 1e-05

def one_map(queries, keys, value_rows):
    factor = HEAD_DIM ** (-0.5)
    scores = jnp.einsum('qhd,khd->hqk', queries.astype(jnp.float32), keys.astype(jnp.float32)) * factor
    row_peak = lax.optimization_barrier(jnp.max(scores, axis=-1, keepdims=True))
    weights = jnp.exp(scores - row_peak)
    totals = lax.optimization_barrier(jnp.sum(weights, axis=-1))
    rounded = lax.optimization_barrier(weights.astype(jnp.bfloat16))
    summed = jnp.einsum('hqk,khe->qhe', rounded.astype(jnp.float32), value_rows.astype(jnp.float32))
    return summed / jnp.transpose(totals)[:, :, None]

def layer_normed(heads_rows, residual_rows, out_weight, norm_gain):
    branch = jnp.dot(heads_rows, out_weight, preferred_element_type=jnp.float32)
    mixed_in = ALPHA * residual_rows.astype(jnp.float32) + branch
    row_mean = lax.optimization_barrier(jnp.mean(mixed_in, axis=-1, keepdims=True))
    centered = mixed_in - row_mean
    row_var = lax.optimization_barrier(jnp.mean(centered * centered, axis=-1, keepdims=True))
    return (centered * lax.rsqrt(row_var + EPSILON) * norm_gain).astype(jnp.bfloat16)

def reference(stream, query_one, key_one, query_two, key_two, values, lambdas, head_gain, out_weight, norm_gain, gate_weight, up_weight, down_weight):
    keys_first = key_one.reshape(SEQ, HEADS, HEAD_DIM)
    keys_second = key_two.reshape(SEQ, HEADS, HEAD_DIM)
    value_rows = values.reshape(SEQ, HEADS, VDIM)
    block_rows = 256
    block_count = SEQ // block_rows

    def attend(position):
        begin_row = position * block_rows
        first_rows = lax.dynamic_slice_in_dim(query_one, begin_row, block_rows, 0).reshape(block_rows, HEADS, HEAD_DIM)
        second_rows = lax.dynamic_slice_in_dim(query_two, begin_row, block_rows, 0).reshape(block_rows, HEADS, HEAD_DIM)
        first_map = one_map(first_rows, keys_first, value_rows)
        second = one_map(second_rows, keys_second, value_rows)
        differ = first_map - lambdas[None, :, None] * second
        inverse_rms = lax.rsqrt(lax.optimization_barrier(jnp.mean(differ * differ, axis=-1, keepdims=True)) + EPSILON)
        return (differ * inverse_rms * head_gain * 0.8).astype(jnp.bfloat16).reshape(block_rows, HEADS * VDIM)
    attended = lax.map(attend, jnp.arange(block_count, dtype=jnp.int32)).reshape(SEQ, HEADS * VDIM)
    normed = layer_normed(attended, stream, out_weight, norm_gain)
    gate_out = jnp.dot(normed, gate_weight, preferred_element_type=jnp.float32)
    upward = jnp.dot(normed, up_weight, preferred_element_type=jnp.float32)
    hidden = (jax.nn.silu(gate_out) * upward).astype(jnp.bfloat16)
    group_width = FF // N_TP
    mixer_out = jnp.zeros((SEQ, D), jnp.float32)
    for group_index in range(N_TP):
        low_unit = group_index * group_width
        partial_value = jnp.dot(hidden[:, low_unit:low_unit + group_width], down_weight[low_unit:low_unit + group_width, :], preferred_element_type=jnp.float32)
        partial_value = lax.optimization_barrier(partial_value.astype(jnp.bfloat16))
        mixer_out = mixer_out + partial_value.astype(jnp.float32)
    return (ALPHA * normed.astype(jnp.float32) + 0.5 * mixer_out).astype(jnp.bfloat16)
```

```python
import functools
import math

import jax
import jax.numpy as jnp
from jax import lax
from jax.experimental import pallas as pl
from jax.experimental.pallas import tpu as pltpu
from jax.sharding import PartitionSpec as P

MESH = pl.DeviceIdType.MESH
F32 = jnp.float32
BF16 = jnp.bfloat16
ALPHA = 1.4142135623730951
EPSILON = 1e-05
SCALE = math.log2(math.e) / 8.0
NB = 4
REL = (2, 1, 3, 0)
Z_OF_SLOT = (0, -1, 1, -2, 2, -3, 3, 4)


class Messages:
    def __init__(self):
        self.index = {}

    def of(self, name):
        return self.index.setdefault(name, len(self.index))


def message_names():
    names = [("q", p) for p in range(3)]
    for a in "kv":
        names += [(a, s) for s in range(1, 8)] + [(a + "d", s) for s in range(8)]
    names += [("t",)] + [("wz", s) for s in range(1, 7)] + [("wz7a",), ("wz7b",)]
    for kind in ("wxl", "wxr", "wxa", "wxb", "wd0", "wd1", "wd2", "wd3"):
        names += [(kind, i) for i in range(8)]
    names += [("s", j) for j in range(1, 4)]
    names += [("o", p) for p in range(3)] + [("st", p) for p in range(3)]
    names += [("a", dy, dx) for dy in range(4) for dx in range(4) if dy or dx]
    names += [("p", h, j) for h in range(2) for j in range(1, 4)]
    return names


NAMES = message_names()
INDEX = {name: i for i, name in enumerate(NAMES)}


def kernel(
    q_ref, k_ref, v_ref, w_ref, s_ref, lam_ref, hg_ref, ng_ref, wo_ref,
    out_ref,
    q_all, k_all, v_all, acc, m_st, l_st, sb0, sb1, w_all, s_all, wo_v,
    o_out, st_out, o_in, st_in, att_own, att, branch, normed, hidden, part, part_in,
    send_sems, recv_sems, local_sems,
):
    sp = lax.axis_index("sp")
    x = lax.axis_index("tp")
    z = sp // 8
    y = lax.rem(sp, 8) // 2
    c = lax.rem(sp, 2)

    def mod(a, n):
        return lax.rem(a + 2 * n, n)

    def at(dz=0, dy=0, dc=0, dx=0):
        return {
            "sp": mod(z + dz, 8) * 8 + mod(y + dy, 4) * 2 + mod(c + dc, 2),
            "tp": mod(x + dx, 4),
        }

    def block(dz=0, dx=0):
        return mod(z + dz, 8) * 8 + mod(x + dx, 4) * 2 + c

    def remote(name, src, dst, target):
        i = INDEX[name]
        return pltpu.make_async_remote_copy(
            src_ref=src, dst_ref=dst, send_sem=send_sems.at[i], recv_sem=recv_sems.at[i],
            device_id=target, device_id_type=MESH,
        )

    def describe(name):
        kind = name[0]
        if kind == "q":
            p = name[1]
            return remote(name, q_ref, q_all.at[p], at(dy=REL[p]))
        if kind in ("k", "v"):
            s = name[1]
            buf, own = (k_all, k_ref) if kind == "k" else (v_all, v_ref)
            step = 1 if s in (1, 3, 5) else -1
            before = s - 2
            if s == 7:
                step, before = (1, 5) if kind == "k" else (-1, 6)
            src = own if s <= 2 else buf.at[2 * before]
            return remote(name, src, buf.at[2 * s], at(dz=step))
        if kind in ("kd", "vd"):
            s = name[1]
            buf, own = (k_all, k_ref) if kind == "kd" else (v_all, v_ref)
            return remote(name, own if s == 0 else buf.at[2 * s], buf.at[2 * s + 1], at(dc=1))
        if kind == "t":
            return remote(name, w_ref, w_all.at[z * 8 + y * 2 + c], {"sp": z * 8 + x * 2 + c, "tp": y})
        if kind == "wz":
            s = name[1]
            step = 1 if s in (1, 3, 5) else -1
            ref = w_all.at[block(dz=Z_OF_SLOT[s - 2] if s > 2 else 0)]
            return remote(name, ref, ref, at(dz=step))
        if kind == "wz7a":
            ref = w_all.at[block(dz=-3), 0:48]
            return remote(name, ref, ref, at(dz=1))
        if kind == "wz7b":
            ref = w_all.at[block(dz=3), 48:96]
            return remote(name, ref, ref, at(dz=-1))
        if kind in ("wxl", "wxr"):
            ref = w_all.at[block(dz=Z_OF_SLOT[name[1]])]
            return remote(name, ref, ref, at(dx=1 if kind == "wxl" else -1))
        if kind == "wxa":
            ref = w_all.at[block(dz=Z_OF_SLOT[name[1]], dx=-1), 0:48]
            return remote(name, ref, ref, at(dx=1))
        if kind == "wxb":
            ref = w_all.at[block(dz=Z_OF_SLOT[name[1]], dx=1), 48:96]
            return remote(name, ref, ref, at(dx=-1))
        if kind[:2] == "wd":
            ref = w_all.at[block(dz=Z_OF_SLOT[name[1]], dx=(0, -1, 1, 2)[int(kind[2])])]
            return remote(name, ref, ref, at(dc=1))
        if kind == "s":
            return remote(name, s_ref, s_all.at[name[1]], at(dy=name[1]))
        if kind == "o":
            p = name[1]
            return remote(name, o_out.at[p], o_in.at[p], at(dy=-REL[p]))
        if kind == "st":
            p = name[1]
            return remote(name, st_out.at[p], st_in.at[p], at(dy=-REL[p]))
        if kind == "a":
            dy, dx = name[1:]
            rows = pl.multiple_of(mod(x + dx, 4) * 64, 64)
            return remote(
                name, att_own.at[pl.ds(rows, 64)], att.at[x, dy * 64:(dy + 1) * 64], at(dy=dy, dx=dx)
            )
        if kind == "p":
            h, j = name[1:]
            return remote(name, part.at[h, j], part_in.at[h, j], at(dy=-j))
        raise KeyError(kind)

    def start(*names):
        for name in names:
            describe(name).start()

    def arrive(*names):
        for name in names:
            describe(name).wait_recv()

    barrier = pltpu.get_barrier_semaphore()
    partners = [at(dz=1), at(dz=-1), at(dc=1)]
    partners += [at(dy=dy, dx=dx) for dy in range(4) for dx in range(4) if dy or dx]
    for partner in partners:
        pl.semaphore_signal(barrier, inc=1, device_id=partner, device_id_type=MESH)
    wo_copy = pltpu.make_async_copy(wo_ref, wo_v, local_sems.at[0])
    wo_copy.start()
    q_all[3] = q_ref[...]
    k_all[0] = k_ref[...]
    v_all[0] = v_ref[...]
    s_all[0] = s_ref[...]
    m_st[...] = jnp.full_like(m_st, -1e30)
    l_st[...] = jnp.zeros_like(l_st)
    acc[...] = jnp.zeros_like(acc)
    pl.semaphore_wait(barrier, len(partners))

    own_w = pltpu.make_async_copy(w_ref, w_all.at[z * 8 + y * 2 + c], local_sems.at[1])
    stays = x == y
    start(("q", 0), ("k", 1), ("k", 2), ("kd", 0), ("v", 1), ("v", 2), ("vd", 0), ("q", 1), ("q", 2))

    @pl.when(stays)
    def _():
        own_w.start()

    @pl.when(jnp.logical_not(stays))
    def _():
        start(("t",))

    @pl.when(stays)
    def _():
        own_w.wait()

    @pl.when(jnp.logical_not(stays))
    def _():
        arrive(("t",))

    start(("wxl", 0), ("wxr", 0), ("wd0", 0))
    arrive(("q", 0), ("kd", 0), ("vd", 0), ("k", 1))
    start(("k", 3), ("kd", 1))
    arrive(("k", 2))
    start(("k", 4), ("kd", 2))
    arrive(("v", 1))
    start(("v", 3), ("vd", 1))
    arrive(("v", 2))
    start(("v", 4), ("vd", 2))
    start(("wz", 1), ("wz", 2))
    arrive(("kd", 1), ("vd", 1))

    def w_across(i):
        def act():
            start(("wxl", i), ("wxr", i), ("wd0", i))
        return act

    def w_on(i):
        def act():
            arrive(("wxl", i), ("wxr", i))
            start(("wxa", i), ("wxb", i), ("wd1", i), ("wd2", i))
        return act

    def w_last(i):
        def act():
            arrive(("wxa", i), ("wxb", i))
            start(("wd3", i))
        return act

    def ring_on(s):
        def act():
            for a in "kv":
                arrive((a, s), (a, s + 1))
                if s < 5:
                    start((a, s + 2), (a, s + 3))
                else:
                    start((a, 7))
                start((a + "d", s), (a + "d", s + 1))
        return act

    def ring_end():
        arrive(("k", 7), ("v", 7))
        start(("kd", 7), ("vd", 7))

    def copies(*slots):
        def act():
            for s in slots:
                arrive(("kd", s), ("vd", s))
        return act

    def w_ring(s):
        def act():
            arrive(("wz", s), ("wz", s + 1))
            if s < 5:
                start(("wz", s + 2), ("wz", s + 3))
            else:
                start(("wz7a",), ("wz7b",))
        return act

    def w_ring_end():
        arrive(("wz7a",), ("wz7b",))

    def finalize(p):
        def act():
            for hm in range(4):
                unit = p * 4 + hm
                total = jnp.sum(l_st[unit], axis=0, keepdims=True)
                o_out[p, hm * 128:(hm + 1) * 128, :] = (acc[unit] * (1.0 / total)).astype(BF16)
                st_out[p, hm:hm + 1, :] = m_st[unit, 0:1, :]
                st_out[p, 4 + hm:5 + hm, :] = total
            start(("o", p), ("st", p))
        return act

    events = {
        0: [lambda: arrive(("q", 1))],
        1: [lambda: arrive(("q", 2)), lambda: start(("s", 1), ("s", 3), ("s", 2))],
        2: [w_on(0)],
        3: [ring_on(3), copies(2, 3)],
        4: [w_ring(1), w_across(1), w_across(2), w_last(0)],
        7: [ring_on(5), copies(4, 5), w_on(1), w_on(2)],
        8: [w_ring(3), w_across(3), w_across(4)],
        10: [w_last(1), w_last(2)],
        11: [ring_end, copies(6, 7), w_on(3), w_on(4)],
        12: [w_ring(5), w_across(5), w_across(6)],
        13: [finalize(0), w_last(3), w_last(4)],
        14: [finalize(1)],
        15: [finalize(2), w_on(5), w_on(6)],
    }

    def scores(s_buf, qi, hm, first):
        m, h = hm // 2, hm % 2
        q = q_all[qi, :, m * 128:(m + 1) * 128]
        lane = lax.broadcasted_iota(jnp.int32, q.shape, 1)
        q = jnp.where((lane >= 64) if h else (lane < 64), q, jnp.zeros_like(q))
        peak = None
        for b in range(NB):
            s = lax.dot_general(
                k_all[first + b, :, m * 128:(m + 1) * 128], q, (((1,), (1,)), ((), ())),
                preferred_element_type=F32,
            )
            s_buf[b * 256:(b + 1) * 256, :] = s
            r = jnp.max(s.reshape(32, 8, 256), axis=0)
            peak = r if peak is None else jnp.maximum(peak, r)
        return peak

    def absorb(s_buf, unit, hm, first, peak):
        h = hm % 2
        m_old = m_st[unit]
        m_new = jnp.maximum(m_old, jnp.max(peak, axis=0, keepdims=True) * SCALE)
        rescale = jnp.exp2(m_old - m_new)
        m_st[unit] = m_new
        total, out = None, None
        for b in range(NB):
            s = s_buf[b * 256:(b + 1) * 256, :].reshape(32, 8, 256)
            weights = jnp.exp2(s * SCALE - m_new[None])
            t = jnp.sum(weights, axis=0)
            total = t if total is None else total + t
            o = jnp.dot(
                v_all[first + b, h * 128:(h + 1) * 128, :], weights.reshape(256, 256).astype(BF16),
                preferred_element_type=F32,
            )
            out = o if out is None else out + o
        l_st[unit] = l_st[unit] * rescale + total
        acc[unit] = (acc[unit].reshape(16, 8, 256) * rescale[None] + out.reshape(16, 8, 256)).reshape(128, 256)

    bufs = (sb0, sb1)
    first_peak = scores(bufs[0], 0, 0, 0)

    def body(t, peak):
        for when, actions in events.items():
            @pl.when(t == when)
            def _(actions=actions):
                for action in actions:
                    action()
        step, qi = t // 4, lax.rem(t, 4)
        later = jnp.minimum(t + 1, 15)
        for hm in range(4):
            if hm < 3:
                ahead = scores(bufs[(hm + 1) % 2], qi, hm + 1, step * NB)
            else:
                ahead = scores(bufs[0], lax.rem(later, 4), 0, (later // 4) * NB)
            absorb(bufs[hm % 2], qi * 4 + hm, hm, step * NB, peak)
            peak = ahead
        return peak

    lax.fori_loop(0, 16, body, first_peak)

    w_ring_end()
    w_across(7)()
    for p in range(3):
        arrive(("o", p), ("st", p))
    for h in range(2):
        maps = []
        for m in range(2):
            hm = m * 2 + h
            unit = 12 + hm
            peaks = [st_in[p, hm:hm + 1, :] for p in range(3)] + [m_st[unit, 0:1, :]]
            sums = [st_in[p, 4 + hm:5 + hm, :] for p in range(3)] + [jnp.sum(l_st[unit], axis=0, keepdims=True)]
            top = functools.reduce(jnp.maximum, peaks)
            powers = [jnp.exp2(v - top) for v in peaks]
            total = sum(v * l for v, l in zip(powers, sums))
            inverse = 1.0 / total
            merged = acc[unit] * (powers[3] * inverse)
            for p in range(3):
                merged += o_in[p, hm * 128:(hm + 1) * 128, :].astype(F32) * (powers[p] * sums[p] * inverse)
            maps.append(merged)
        differ = maps[0] - lam_ref[h] * maps[1]
        mean_square = jnp.mean(differ * differ, axis=0, keepdims=True)
        scaled = jnp.transpose(differ * lax.rsqrt(mean_square + EPSILON))
        att_own[:, h * 128:(h + 1) * 128] = (scaled * hg_ref[...] * 0.8).astype(BF16)
    exchange = [("a", dy, dx) for dy in range(4) for dx in range(4) if dy or dx]
    rows = pl.multiple_of(x * 64, 64)
    keep = pltpu.make_async_copy(att_own.at[pl.ds(rows, 64)], att.at[x, 0:64], local_sems.at[2])
    keep.start()
    start(*exchange)
    w_last(5)()
    w_last(6)()
    w_on(7)()
    keep.wait()
    wo_copy.wait()
    arrive(*exchange)

    def project(n, carry):
        cols = pl.ds(pl.multiple_of(n * 256, 256), 256)
        total = None
        for i in range(4):
            term = jnp.dot(att[i], wo_v[i * 256:(i + 1) * 256, cols], preferred_element_type=F32)
            total = term if total is None else total + term
        branch[:, cols] = total
        return carry

    lax.fori_loop(0, 8, project, 0)
    w_last(7)()
    arrive(("s", 1), ("s", 2), ("s", 3))

    def norm(n, carry):
        r = pl.ds(pl.multiple_of(n * 16, 16), 16)
        j, within = n // 4, pl.ds(pl.multiple_of(lax.rem(n, 4) * 16, 16), 16)
        mixed = ALPHA * s_all[j, within, :].astype(F32) + branch[r, :]
        mean = jnp.mean(mixed, axis=-1, keepdims=True)
        centered = mixed - mean
        var = jnp.mean(centered * centered, axis=-1, keepdims=True)
        normed[r, :] = (centered * lax.rsqrt(var + EPSILON) * ng_ref[...]).astype(BF16)
        return carry

    lax.fori_loop(0, 16, norm, 0)
    for kind in ("wd0", "wd1", "wd2", "wd3"):
        arrive(*[(kind, i) for i in range(8)])
    for lo, hi in ((0, 256), (256, 512), (512, 704)):
        gate = jnp.dot(normed[...], w_all[:, 0:32, lo:hi].reshape(2048, hi - lo), preferred_element_type=F32)
        upward = jnp.dot(normed[...], w_all[:, 32:64, lo:hi].reshape(2048, hi - lo), preferred_element_type=F32)
        hidden[:, lo:hi] = (gate / (1.0 + jnp.exp(-gate)) * upward).astype(BF16)
    for h in range(2):
        def down(n, carry):
            rows_of = pl.ds(pl.multiple_of((h * 4 + n) * 8, 8), 8)
            product = lax.dot_general(
                hidden[...], w_all[rows_of, 64:96, :].reshape(256, 704), (((1,), (1,)), ((), ())),
                preferred_element_type=F32,
            ).astype(BF16)
            cols = pl.ds(pl.multiple_of(n * 256, 256), 256)
            for j in range(4):
                part[h, j, :, cols] = product[j * 64:(j + 1) * 64]
            return carry

        lax.fori_loop(0, 4, down, 0)
        start(("p", h, 2), ("p", h, 1), ("p", h, 3))
    for h in range(2):
        for j in range(1, 4):
            arrive(("p", h, j))
        cols = slice(h * 1024, (h + 1) * 1024)
        mixer = part[h, 0].astype(F32)
        for j in range(1, 4):
            mixer += part_in[h, j].astype(F32)
        out_ref[:, cols] = (ALPHA * normed[0:64, cols].astype(F32) + 0.5 * mixer).astype(BF16)
    for name in NAMES:
        if name != ("t",):
            describe(name).wait_send()

    @pl.when(jnp.logical_not(stays))
    def _():
        describe(("t",)).wait_send()


def on_device(
    stream, query_one, key_one, query_two, key_two, values, lambdas, head_gain, out_weight, norm_gain,
    gate_weight, up_weight, down_weight,
):
    queries = jnp.concatenate([query_one, query_two], axis=1)
    keys = jnp.concatenate([key_one, key_two], axis=1)
    turned = jnp.transpose(values)
    weights = jnp.concatenate([gate_weight, up_weight, jnp.transpose(down_weight)], axis=0)
    vmem = pl.BlockSpec(memory_space=pltpu.VMEM)
    return pl.pallas_call(
        kernel,
        out_shape=jax.ShapeDtypeStruct((64, 2048), BF16),
        in_specs=[vmem] * 5 + [pl.BlockSpec(memory_space=pltpu.SMEM), vmem, vmem, pl.BlockSpec(memory_space=pl.ANY)],
        out_specs=vmem,
        scratch_shapes=[
            pltpu.VMEM((4, 256, 256), BF16),
            pltpu.VMEM((16, 256, 256), BF16),
            pltpu.VMEM((16, 256, 256), BF16),
            pltpu.VMEM((16, 128, 256), F32),
            pltpu.VMEM((16, 8, 256), F32),
            pltpu.VMEM((16, 8, 256), F32),
            pltpu.VMEM((NB * 256, 256), F32),
            pltpu.VMEM((NB * 256, 256), F32),
            pltpu.VMEM((64, 96, 704), BF16),
            pltpu.VMEM((4, 64, 2048), BF16),
            pltpu.VMEM((1024, 2048), BF16),
            pltpu.VMEM((3, 512, 256), BF16),
            pltpu.VMEM((3, 8, 256), F32),
            pltpu.VMEM((3, 512, 256), BF16),
            pltpu.VMEM((3, 8, 256), F32),
            pltpu.VMEM((256, 256), BF16),
            pltpu.VMEM((4, 256, 256), BF16),
            pltpu.VMEM((256, 2048), F32),
            pltpu.VMEM((256, 2048), BF16),
            pltpu.VMEM((256, 704), BF16),
            pltpu.VMEM((2, 4, 64, 1024), BF16),
            pltpu.VMEM((2, 4, 64, 1024), BF16),
            pltpu.SemaphoreType.DMA((len(NAMES),)),
            pltpu.SemaphoreType.DMA((len(NAMES),)),
            pltpu.SemaphoreType.DMA((3,)),
        ],
        compiler_params=pltpu.CompilerParams(
            collective_id=0, has_side_effects=True, vmem_limit_bytes=60 * 2**20
        ),
    )(
        queries, keys, turned, weights, stream, lambdas, head_gain.reshape(1, 128), norm_gain.reshape(1, 2048),
        out_weight,
    )


def solution(mesh):
    return jax.shard_map(
        on_device,
        mesh=mesh,
        in_specs=(
            P(("sp", "tp"), None), P("sp", "tp"), P("sp", "tp"), P("sp", "tp"), P("sp", "tp"), P("sp", "tp"),
            P("tp"), P(), P(), P(), P("sp", "tp"), P("sp", "tp"), P("tp", "sp"),
        ),
        out_specs=P(("sp", "tp"), None),
        check_vma=False,
    )
```

```python
import functools
import math

import jax
import jax.numpy as jnp
from jax import lax
from jax.experimental import pallas as pl
from jax.experimental.pallas import tpu as pltpu
from jax.sharding import PartitionSpec as P

MESH = pl.DeviceIdType.MESH
F32 = jnp.float32
BF16 = jnp.bfloat16
ALPHA = 1.4142135623730951
EPSILON = 1e-05
SCALE = math.log2(math.e) / 8.0
NB = 2
REL = (2, 1, 3, 0)
Z_OF_SLOT = (0, -1, 1, -2, 2, -3, 3, 4)


def message_names():
    names = [("q", p) for p in range(3)]
    for a in "kv":
        names += [(a, s) for s in range(1, 8)] + [(a + "d", s) for s in range(8)]
    names += [("t",)] + [("wz", s) for s in range(1, 7)] + [("wz7a",), ("wz7b",)]
    for kind in ("wxl", "wxr", "wxa", "wxb", "wd0", "wd1", "wd2", "wd3"):
        names += [(kind, i) for i in range(8)]
    names += [("s", j) for j in range(1, 4)]
    names += [("o", p) for p in range(3)] + [("st", p) for p in range(3)]
    names += [("a", dy, dx) for dy in range(4) for dx in range(4) if dy or dx]
    names += [("p", h, j) for h in range(2) for j in range(1, 4)]
    return names


NAMES = message_names()
INDEX = {name: i for i, name in enumerate(NAMES)}


def kernel(
    q1_ref, q2_ref, k1_ref, k2_ref, v_ref, g_ref, u_ref, d_ref, s_ref, lam_ref, hg_ref, ng_ref, wo_ref,
    out_ref,
    q_all, k_all, v_all, acc, m_st, l_st, sb0, sb1, w_own, w_all, s_all, wo_v,
    o_out, st_out, o_in, st_in, att_own, att, branch, row_sums, normed, hidden, part, part_in,
    send_sems, recv_sems, local_sems,
):
    sp = lax.axis_index("sp")
    x = lax.axis_index("tp")
    z = sp // 8
    y = lax.rem(sp, 8) // 2
    c = lax.rem(sp, 2)

    def mod(a, n):
        return lax.rem(a + 2 * n, n)

    def at(dz=0, dy=0, dc=0, dx=0):
        return {
            "sp": mod(z + dz, 8) * 8 + mod(y + dy, 4) * 2 + mod(c + dc, 2),
            "tp": mod(x + dx, 4),
        }

    def block(dz=0, dx=0):
        return mod(z + dz, 8) * 8 + mod(x + dx, 4) * 2 + c

    def remote(name, src, dst, target):
        i = INDEX[name]
        return pltpu.make_async_remote_copy(
            src_ref=src, dst_ref=dst, send_sem=send_sems.at[i], recv_sem=recv_sems.at[i],
            device_id=target, device_id_type=MESH,
        )

    def describe(name):
        kind = name[0]
        if kind == "q":
            p = name[1]
            return remote(name, q_all.at[3], q_all.at[p], at(dy=REL[p]))
        if kind in ("k", "v"):
            s = name[1]
            buf = k_all if kind == "k" else v_all
            step = 1 if s in (1, 3, 5) else -1
            before = s - 2
            if s == 7:
                step, before = (1, 5) if kind == "k" else (-1, 6)
            return remote(name, buf.at[2 * max(before, 0)], buf.at[2 * s], at(dz=step))
        if kind in ("kd", "vd"):
            s = name[1]
            buf = k_all if kind == "kd" else v_all
            return remote(name, buf.at[2 * s], buf.at[2 * s + 1], at(dc=1))
        if kind == "t":
            return remote(name, w_own, w_all.at[z * 8 + y * 2 + c], {"sp": z * 8 + x * 2 + c, "tp": y})
        if kind == "wz":
            s = name[1]
            step = 1 if s in (1, 3, 5) else -1
            ref = w_all.at[block(dz=Z_OF_SLOT[s - 2] if s > 2 else 0)]
            return remote(name, ref, ref, at(dz=step))
        if kind == "wz7a":
            ref = w_all.at[block(dz=-3), 0:48]
            return remote(name, ref, ref, at(dz=1))
        if kind == "wz7b":
            ref = w_all.at[block(dz=3), 48:96]
            return remote(name, ref, ref, at(dz=-1))
        if kind in ("wxl", "wxr"):
            ref = w_all.at[block(dz=Z_OF_SLOT[name[1]])]
            return remote(name, ref, ref, at(dx=1 if kind == "wxl" else -1))
        if kind == "wxa":
            ref = w_all.at[block(dz=Z_OF_SLOT[name[1]], dx=-1), 0:48]
            return remote(name, ref, ref, at(dx=1))
        if kind == "wxb":
            ref = w_all.at[block(dz=Z_OF_SLOT[name[1]], dx=1), 48:96]
            return remote(name, ref, ref, at(dx=-1))
        if kind[:2] == "wd":
            ref = w_all.at[block(dz=Z_OF_SLOT[name[1]], dx=(0, -1, 1, 2)[int(kind[2])])]
            return remote(name, ref, ref, at(dc=1))
        if kind == "s":
            return remote(name, s_ref, s_all.at[name[1]], at(dy=name[1]))
        if kind == "o":
            p = name[1]
            return remote(name, o_out.at[p], o_in.at[p], at(dy=-REL[p]))
        if kind == "st":
            p = name[1]
            return remote(name, st_out.at[p], st_in.at[p], at(dy=-REL[p]))
        if kind == "a":
            dy, dx = name[1:]
            rows = pl.multiple_of(mod(x + dx, 4) * 64, 64)
            return remote(
                name, att_own.at[pl.ds(rows, 64)], att.at[x, dy * 64:(dy + 1) * 64], at(dy=dy, dx=dx)
            )
        if kind == "p":
            h, j = name[1:]
            return remote(name, part.at[h, j], part_in.at[h, j], at(dy=-j))
        raise KeyError(kind)

    def start(*names):
        for name in names:
            describe(name).start()

    def arrive(*names):
        for name in names:
            describe(name).wait_recv()

    barrier = pltpu.get_barrier_semaphore()
    partners = [at(dz=1), at(dz=-1), at(dc=1)]
    partners += [at(dy=dy, dx=dx) for dy in range(4) for dx in range(4) if dy or dx]
    for partner in partners:
        pl.semaphore_signal(barrier, inc=1, device_id=partner, device_id_type=MESH)
    wo_copy = pltpu.make_async_copy(wo_ref, wo_v, local_sems.at[0])
    wo_copy.start()
    q_all[3, :, 0:128] = q1_ref[...]
    q_all[3, :, 128:256] = q2_ref[...]
    k_all[0, :, 0:128] = k1_ref[...]
    k_all[0, :, 128:256] = k2_ref[...]
    v_all[0] = jnp.transpose(v_ref[...])
    w_own[0:32] = g_ref[...]
    w_own[32:64] = u_ref[...]
    w_own[64:96] = d_ref[...]
    s_all[0] = s_ref[...]
    m_st[...] = jnp.full_like(m_st, -1e30)
    l_st[...] = jnp.zeros_like(l_st)
    acc[...] = jnp.zeros_like(acc)
    pl.semaphore_wait(barrier, len(partners))

    own_w = pltpu.make_async_copy(w_own, w_all.at[z * 8 + y * 2 + c], local_sems.at[1])
    stays = x == y
    start(("q", 0), ("k", 1), ("k", 2), ("kd", 0), ("v", 1), ("v", 2), ("vd", 0), ("q", 1), ("q", 2))

    @pl.when(stays)
    def _():
        own_w.start()

    @pl.when(jnp.logical_not(stays))
    def _():
        start(("t",))

    arrive(("q", 0), ("kd", 0), ("vd", 0))

    def w_in():
        @pl.when(stays)
        def _():
            own_w.wait()

        @pl.when(jnp.logical_not(stays))
        def _():
            arrive(("t",))

        start(("wz", 1), ("wz", 2))

    def w_across(i):
        def act():
            start(("wxl", i), ("wxr", i), ("wd0", i))
        return act

    def w_on(i):
        def act():
            arrive(("wxl", i), ("wxr", i))
            start(("wxa", i), ("wxb", i), ("wd1", i), ("wd2", i))
        return act

    def w_last(i):
        def act():
            arrive(("wxa", i), ("wxb", i))
            start(("wd3", i))
        return act

    def on(a, s):
        def act():
            arrive((a, s), (a, s + 1))
            if s < 5:
                start((a, s + 2), (a, s + 3))
            else:
                start((a, 7))
            start((a + "d", s), (a + "d", s + 1))
        return act

    def ring_end():
        arrive(("k", 7), ("v", 7))
        start(("kd", 7), ("vd", 7))

    def got(*names):
        return lambda: arrive(*names)

    def w_ring(s):
        def act():
            arrive(("wz", s), ("wz", s + 1))
            if s < 5:
                start(("wz", s + 2), ("wz", s + 3))
            else:
                start(("wz7a",), ("wz7b",))
            w_across(s)()
            w_across(s + 1)()
        return act

    def w_ring_end():
        arrive(("wz7a",), ("wz7b",))

    def finalize(p):
        def act():
            for hm in range(4):
                unit = p * 4 + hm
                total = jnp.sum(l_st[unit], axis=0, keepdims=True)
                o_out[p, hm * 128:(hm + 1) * 128, :] = (acc[unit] * (1.0 / total)).astype(BF16)
                st_out[p, hm:hm + 1, :] = m_st[unit, 0:1, :]
                st_out[p, 4 + hm:5 + hm, :] = total
            start(("o", p), ("st", p))
        return act

    events = {
        0: [got(("q", 1))],
        1: [got(("q", 2)), on("k", 1)],
        2: [lambda: start(("s", 1), ("s", 3), ("s", 2))],
        3: [on("v", 1), got(("kd", 1))],
        4: [got(("vd", 1)), w_in, w_across(0)],
        7: [got(("kd", 2), ("vd", 2)), on("k", 3)],
        10: [on("v", 3)],
        11: [got(("kd", 3), ("vd", 3))],
        12: [w_on(0)],
        15: [w_ring(1), got(("kd", 4), ("vd", 4))],
        18: [on("k", 5)],
        19: [on("v", 5), got(("kd", 5), ("vd", 5))],
        20: [w_last(0)],
        22: [w_on(1)],
        23: [got(("kd", 6), ("vd", 6)), ring_end],
        24: [got(("kd", 7), ("vd", 7)), w_on(2)],
        26: [finalize(0)],
        27: [w_ring(3), w_last(1)],
        28: [finalize(1)],
        30: [finalize(2), w_last(2)],
    }

    def scores(s_buf, qi, hm, first):
        m, h = hm // 2, hm % 2
        q = q_all[qi, :, m * 128:(m + 1) * 128]
        lane = lax.broadcasted_iota(jnp.int32, q.shape, 1)
        q = jnp.where((lane >= 64) if h else (lane < 64), q, jnp.zeros_like(q))
        peak = None
        for b in range(NB):
            s = lax.dot_general(
                k_all[first + b, :, m * 128:(m + 1) * 128], q, (((1,), (1,)), ((), ())),
                preferred_element_type=F32,
            )
            s_buf[b * 256:(b + 1) * 256, :] = s
            r = jnp.max(s.reshape(32, 8, 256), axis=0)
            peak = r if peak is None else jnp.maximum(peak, r)
        return peak

    def absorb(s_buf, unit, hm, first, peak):
        h = hm % 2
        m_old = m_st[unit]
        m_new = jnp.maximum(m_old, jnp.max(peak, axis=0, keepdims=True) * SCALE)
        rescale = jnp.exp2(m_old - m_new)
        m_st[unit] = m_new
        total, out = None, None
        for b in range(NB):
            s = s_buf[b * 256:(b + 1) * 256, :].reshape(32, 8, 256)
            weights = jnp.exp2(s * SCALE - m_new[None])
            t = jnp.sum(weights, axis=0)
            total = t if total is None else total + t
            o = jnp.dot(
                v_all[first + b, h * 128:(h + 1) * 128, :], weights.reshape(256, 256).astype(BF16),
                preferred_element_type=F32,
            )
            out = o if out is None else out + o
        l_st[unit] = l_st[unit] * rescale + total
        acc[unit] = (acc[unit].reshape(16, 8, 256) * rescale[None] + out.reshape(16, 8, 256)).reshape(128, 256)

    bufs = (sb0, sb1)

    def place(t):
        late = t >= 24
        return jnp.where(late, 6 + lax.rem(t, 2), t // 4), jnp.where(late, (t - 24) // 2, lax.rem(t, 4))

    first_peak = scores(bufs[0], 0, 0, 0)

    def body(t, peak):
        for when, actions in events.items():
            @pl.when(t == when)
            def _(actions=actions):
                for action in actions:
                    action()
        slot, qi = place(t)
        slot_ahead, qi_ahead = place(jnp.minimum(t + 1, 31))
        for hm in range(4):
            if hm < 3:
                ahead = scores(bufs[(hm + 1) % 2], qi, hm + 1, slot * NB)
            else:
                ahead = scores(bufs[0], qi_ahead, 0, slot_ahead * NB)
            absorb(bufs[hm % 2], qi * 4 + hm, hm, slot * NB, peak)
            peak = ahead
        return peak

    lax.fori_loop(0, 32, body, first_peak)

    arrive(("o", 0), ("st", 0))
    w_ring(5)()
    arrive(("o", 1), ("st", 1))
    w_on(3)()
    w_on(4)()
    arrive(("o", 2), ("st", 2))
    for h in range(2):
        maps = []
        for m in range(2):
            hm = m * 2 + h
            unit = 12 + hm
            peaks = [st_in[p, hm:hm + 1, :] for p in range(3)] + [m_st[unit, 0:1, :]]
            sums = [st_in[p, 4 + hm:5 + hm, :] for p in range(3)] + [jnp.sum(l_st[unit], axis=0, keepdims=True)]
            top = functools.reduce(jnp.maximum, peaks)
            powers = [jnp.exp2(v - top) for v in peaks]
            total = sum(v * l for v, l in zip(powers, sums))
            inverse = 1.0 / total
            merged = acc[unit] * (powers[3] * inverse)
            for p in range(3):
                merged += o_in[p, hm * 128:(hm + 1) * 128, :].astype(F32) * (powers[p] * sums[p] * inverse)
            maps.append(merged)
        differ = maps[0] - lam_ref[h] * maps[1]
        mean_square = jnp.mean(differ * differ, axis=0, keepdims=True)
        scaled = jnp.transpose(differ * lax.rsqrt(mean_square + EPSILON))
        att_own[:, h * 128:(h + 1) * 128] = (scaled * hg_ref[...] * 0.8).astype(BF16)
    exchange = [("a", dy, dx) for dy in range(4) for dx in range(4) if dy or dx]
    rows = pl.multiple_of(x * 64, 64)
    keep = pltpu.make_async_copy(att_own.at[pl.ds(rows, 64)], att.at[x, 0:64], local_sems.at[2])
    keep.start()
    start(*exchange)
    w_ring_end()
    w_across(7)()
    w_last(3)()
    w_last(4)()
    w_on(5)()
    w_on(6)()
    keep.wait()
    wo_copy.wait()
    arrive(*exchange)

    arrive(("s", 1), ("s", 2), ("s", 3))
    row_sums[...] = jnp.zeros_like(row_sums)

    def project(n, carry):
        cols = pl.ds(pl.multiple_of(n * 512, 512), 512)
        total = None
        for i in range(4):
            term = jnp.dot(att[i], wo_v[i * 256:(i + 1) * 256, cols], preferred_element_type=F32)
            total = term if total is None else total + term
        mixed = ALPHA * s_all[:, :, cols].reshape(256, 512).astype(F32) + total
        branch[:, cols] = mixed
        row_sums[...] += sum(mixed[:, i * 128:(i + 1) * 128] for i in range(4))
        return carry

    lax.fori_loop(0, 4, project, 0)
    w_last(5)()
    w_last(6)()
    w_on(7)()
    mean = jnp.sum(row_sums[...], axis=-1, keepdims=True) * (1.0 / 2048)
    row_sums[...] = jnp.broadcast_to(mean, (256, 128))
    spread = None
    for n in range(16):
        centered = branch[:, n * 128:(n + 1) * 128] - row_sums[...]
        spread = centered * centered if spread is None else spread + centered * centered
    var = jnp.sum(spread, axis=-1, keepdims=True) * (1.0 / 2048)
    inverse = jnp.broadcast_to(lax.rsqrt(var + EPSILON), (256, 128))
    for n in range(16):
        cols = slice(n * 128, (n + 1) * 128)
        normed[:, cols] = ((branch[:, cols] - row_sums[...]) * inverse * ng_ref[:, cols]).astype(BF16)
    w_last(7)()
    for kind in ("wd0", "wd1", "wd2", "wd3"):
        arrive(*[(kind, i) for i in range(8)])
    for lo, hi in ((0, 256), (256, 512), (512, 704)):
        gate = jnp.dot(normed[...], w_all[:, 0:32, lo:hi].reshape(2048, hi - lo), preferred_element_type=F32)
        upward = jnp.dot(normed[...], w_all[:, 32:64, lo:hi].reshape(2048, hi - lo), preferred_element_type=F32)
        hidden[:, lo:hi] = (gate / (1.0 + jnp.exp(-gate)) * upward).astype(BF16)
    for h in range(2):
        def down(n, carry):
            rows_of = pl.ds(pl.multiple_of((h * 4 + n) * 8, 8), 8)
            product = lax.dot_general(
                hidden[...], w_all[rows_of, 64:96, :].reshape(256, 704), (((1,), (1,)), ((), ())),
                preferred_element_type=F32,
            ).astype(BF16)
            cols = pl.ds(pl.multiple_of(n * 256, 256), 256)
            for j in range(4):
                part[h, j, :, cols] = product[j * 64:(j + 1) * 64]
            return carry

        lax.fori_loop(0, 4, down, 0)
        start(("p", h, 2), ("p", h, 1), ("p", h, 3))
    for h in range(2):
        for j in range(1, 4):
            arrive(("p", h, j))
        cols = slice(h * 1024, (h + 1) * 1024)
        mixer = part[h, 0].astype(F32)
        for j in range(1, 4):
            mixer += part_in[h, j].astype(F32)
        out_ref[:, cols] = (ALPHA * normed[0:64, cols].astype(F32) + 0.5 * mixer).astype(BF16)
    for name in NAMES:
        if name != ("t",):
            describe(name).wait_send()

    @pl.when(jnp.logical_not(stays))
    def _():
        describe(("t",)).wait_send()


def on_device(
    stream, query_one, key_one, query_two, key_two, values, lambdas, head_gain, out_weight, norm_gain,
    gate_weight, up_weight, down_weight,
):
    vmem = pl.BlockSpec(memory_space=pltpu.VMEM)
    return pl.pallas_call(
        kernel,
        out_shape=jax.ShapeDtypeStruct((64, 2048), BF16),
        in_specs=[vmem] * 9 + [pl.BlockSpec(memory_space=pltpu.SMEM), vmem, vmem, pl.BlockSpec(memory_space=pl.ANY)],
        out_specs=vmem,
        scratch_shapes=[
            pltpu.VMEM((4, 256, 256), BF16),
            pltpu.VMEM((16, 256, 256), BF16),
            pltpu.VMEM((16, 256, 256), BF16),
            pltpu.VMEM((16, 128, 256), F32),
            pltpu.VMEM((16, 8, 256), F32),
            pltpu.VMEM((16, 8, 256), F32),
            pltpu.VMEM((NB * 256, 256), F32),
            pltpu.VMEM((NB * 256, 256), F32),
            pltpu.VMEM((96, 704), BF16),
            pltpu.VMEM((64, 96, 704), BF16),
            pltpu.VMEM((4, 64, 2048), BF16),
            pltpu.VMEM((1024, 2048), BF16),
            pltpu.VMEM((3, 512, 256), BF16),
            pltpu.VMEM((3, 8, 256), F32),
            pltpu.VMEM((3, 512, 256), BF16),
            pltpu.VMEM((3, 8, 256), F32),
            pltpu.VMEM((256, 256), BF16),
            pltpu.VMEM((4, 256, 256), BF16),
            pltpu.VMEM((256, 2048), F32),
            pltpu.VMEM((256, 128), F32),
            pltpu.VMEM((256, 2048), BF16),
            pltpu.VMEM((256, 704), BF16),
            pltpu.VMEM((2, 4, 64, 1024), BF16),
            pltpu.VMEM((2, 4, 64, 1024), BF16),
            pltpu.SemaphoreType.DMA((len(NAMES),)),
            pltpu.SemaphoreType.DMA((len(NAMES),)),
            pltpu.SemaphoreType.DMA((3,)),
        ],
        compiler_params=pltpu.CompilerParams(
            collective_id=0, has_side_effects=True, vmem_limit_bytes=60 * 2**20
        ),
    )(
        query_one, query_two, key_one, key_two, values, gate_weight, up_weight, jnp.transpose(down_weight), stream, lambdas, head_gain.reshape(1, 128), norm_gain.reshape(1, 2048),
        out_weight,
    )


def solution(mesh):
    return jax.shard_map(
        on_device,
        mesh=mesh,
        in_specs=(
            P(("sp", "tp"), None), P("sp", "tp"), P("sp", "tp"), P("sp", "tp"), P("sp", "tp"), P("sp", "tp"),
            P("tp"), P(), P(), P(), P("sp", "tp"), P("sp", "tp"), P("tp", "sp"),
        ),
        out_specs=P(("sp", "tp"), None),
        check_vma=False,
    )
```

```python
import functools
import math

import jax
import jax.numpy as jnp
from jax import lax
from jax.experimental import pallas as pl
from jax.experimental.pallas import tpu as pltpu
from jax.sharding import PartitionSpec as P

MESH = pl.DeviceIdType.MESH
F32 = jnp.float32
BF16 = jnp.bfloat16
ALPHA = 1.4142135623730951
EPSILON = 1e-05
SCALE = math.log2(math.e) / 8.0
REL = (0, 1, 3, 2)
Z_OF_SLOT = (0, -1, 1, -2, 2, -3, 3, 4)


def message_names():
    names = [("q", p) for p in range(1, 4)]
    for a in "kv":
        names += [(a, s) for s in range(1, 8)] + [(a + "d", s) for s in range(8)]
    names += [("wz", s) for s in range(1, 7)] + [("wz7a",), ("wz7b",)]
    for kind in ("wxl", "wxr", "wxa", "wxb", "wd0", "wd1", "wd2", "wd3"):
        names += [(kind, i) for i in range(8)]
    names += [("s", j) for j in range(1, 4)]
    names += [("o", p) for p in range(1, 4)] + [("st", p) for p in range(1, 4)]
    names += [("a", j) for j in range(1, 4)]
    names += [("p", h, j) for h in range(2) for j in range(1, 4)]
    return names


NAMES = message_names()
INDEX = {name: i for i, name in enumerate(NAMES)}


def kernel(
    q1_ref, q2_ref, k1_ref, k2_ref, v_ref, g_ref, u_ref, d_ref, s_ref, lam_ref, hg_ref, ng_ref, wo_ref,
    out_ref,
    q_all, k_all, v_all, v_own, acc, m_st, l_st, sb0, sb1, w_all, s_all, wo_v,
    o_out, st_out, o_in, st_in, att, branch, row_sums, normed, hidden, part, part_in,
    send_sems, recv_sems, local_sems,
):
    sp = lax.axis_index("sp")
    x = lax.axis_index("tp")
    z = sp // 8
    y = lax.rem(sp, 8) // 2
    c = lax.rem(sp, 2)

    def mod(a, n):
        return lax.rem(a + 2 * n, n)

    def at(dz=0, dy=0, dc=0, dx=0):
        return {
            "sp": mod(z + dz, 8) * 8 + mod(y + dy, 4) * 2 + mod(c + dc, 2),
            "tp": mod(x + dx, 4),
        }

    def block(dz=0, dy=0):
        return mod(z + dz, 8) * 8 + mod(y + dy, 4) * 2 + c

    def remote(name, src, dst, target):
        i = INDEX[name]
        return pltpu.make_async_remote_copy(
            src_ref=src, dst_ref=dst, send_sem=send_sems.at[i], recv_sem=recv_sems.at[i],
            device_id=target, device_id_type=MESH,
        )

    def describe(name):
        kind = name[0]
        if kind == "q":
            p = name[1]
            return remote(name, q_all.at[0], q_all.at[p], at(dy=REL[p]))
        if kind in ("k", "v"):
            s = name[1]
            buf = k_all if kind == "k" else v_all
            step = 1 if s in (1, 3, 5) else -1
            before = s - 2
            if s == 7:
                step, before = (1, 5) if kind == "k" else (-1, 6)
            return remote(name, buf.at[2 * max(before, 0)], buf.at[2 * s], at(dz=step))
        if kind in ("kd", "vd"):
            s = name[1]
            buf = k_all if kind == "kd" else v_all
            return remote(name, buf.at[2 * s], buf.at[2 * s + 1], at(dc=1))
        if kind == "wz":
            s = name[1]
            step = 1 if s in (1, 3, 5) else -1
            ref = w_all.at[block(dz=Z_OF_SLOT[s - 2] if s > 2 else 0)]
            return remote(name, ref, ref, at(dz=step))
        if kind == "wz7a":
            ref = w_all.at[block(dz=-3), 0:48]
            return remote(name, ref, ref, at(dz=1))
        if kind == "wz7b":
            ref = w_all.at[block(dz=3), 48:96]
            return remote(name, ref, ref, at(dz=-1))
        if kind in ("wxl", "wxr"):
            ref = w_all.at[block(dz=Z_OF_SLOT[name[1]])]
            return remote(name, ref, ref, at(dy=1 if kind == "wxl" else -1))
        if kind == "wxa":
            ref = w_all.at[block(dz=Z_OF_SLOT[name[1]], dy=-1), 0:48]
            return remote(name, ref, ref, at(dy=1))
        if kind == "wxb":
            ref = w_all.at[block(dz=Z_OF_SLOT[name[1]], dy=1), 48:96]
            return remote(name, ref, ref, at(dy=-1))
        if kind[:2] == "wd":
            ref = w_all.at[block(dz=Z_OF_SLOT[name[1]], dy=(0, -1, 1, 2)[int(kind[2])])]
            return remote(name, ref, ref, at(dc=1))
        if kind == "s":
            return remote(name, s_all.at[x], s_all.at[x], at(dx=name[1]))
        if kind == "o":
            p = name[1]
            return remote(name, o_out.at[p - 1], o_in.at[p - 1], at(dy=-REL[p]))
        if kind == "st":
            p = name[1]
            return remote(name, st_out.at[p - 1], st_in.at[p - 1], at(dy=-REL[p]))
        if kind == "a":
            return remote(name, att.at[x], att.at[x], at(dx=name[1]))
        if kind == "p":
            h, j = name[1:]
            rows = pl.multiple_of(mod(x - j, 4) * 64, 64)
            return remote(name, part.at[h, pl.ds(rows, 64)], part_in.at[h, j], at(dx=-j))
        raise KeyError(kind)

    def start(*names):
        for name in names:
            describe(name).start()

    def arrive(*names):
        for name in names:
            describe(name).wait_recv()

    barrier = pltpu.get_barrier_semaphore()
    partners = [at(dz=1), at(dz=-1), at(dc=1)]
    partners += [at(dy=j) for j in range(1, 4)] + [at(dx=j) for j in range(1, 4)]
    for partner in partners:
        pl.semaphore_signal(barrier, inc=1, device_id=partner, device_id_type=MESH)
    takes = [
        pltpu.make_async_copy(src, dst, local_sems.at[3 + i])
        for i, (src, dst) in enumerate((
            (v_ref, v_own), (q1_ref, q_all.at[0, :, 0:128]), (q2_ref, q_all.at[0, :, 128:256]),
            (k1_ref, k_all.at[0, :, 0:128]), (k2_ref, k_all.at[0, :, 128:256]),
            (g_ref, w_all.at[sp, 0:32]), (u_ref, w_all.at[sp, 32:64]), (d_ref, w_all.at[sp, 64:96]), (s_ref, s_all.at[x]),
        ))
    ]
    for take in takes:
        take.start()
    wo_copy = pltpu.make_async_copy(wo_ref, wo_v, local_sems.at[0])
    wo_copy.start()
    m_st[...] = jnp.full_like(m_st, -1e30)
    l_st[...] = jnp.zeros_like(l_st)
    acc[...] = jnp.zeros_like(acc)
    takes[0].wait()
    v_all[0] = jnp.transpose(v_own[...])
    for take in takes[1:]:
        take.wait()
    pl.semaphore_wait(barrier, len(partners))

    start(("q", 1), ("q", 2), ("kd", 0), ("k", 1), ("k", 2), ("vd", 0), ("v", 1), ("v", 2), ("q", 3))

    def w_across(i):
        def act():
            start(("wxl", i), ("wxr", i), ("wd0", i))
        return act

    def w_on(i):
        def act():
            arrive(("wxl", i), ("wxr", i))
            start(("wxa", i), ("wxb", i), ("wd1", i), ("wd2", i))
        return act

    def w_last(i):
        def act():
            arrive(("wxa", i), ("wxb", i))
            start(("wd3", i))
        return act

    def on(a, s):
        def act():
            arrive((a, s), (a, s + 1))
            if s < 5:
                start((a, s + 2), (a, s + 3))
            else:
                start((a, 7))
            start((a + "d", s), (a + "d", s + 1))
        return act

    def ring_end():
        arrive(("k", 7), ("v", 7))
        start(("kd", 7), ("vd", 7))

    def got(*names):
        return lambda: arrive(*names)

    def w_ring(s):
        def act():
            arrive(("wz", s), ("wz", s + 1))
            w_across(s)()
            w_across(s + 1)()
        return act

    def w_next(s):
        def act():
            if s < 5:
                start(("wz", s + 2), ("wz", s + 3))
            else:
                start(("wz7a",), ("wz7b",))
        return act

    def w_ring_end():
        arrive(("wz7a",), ("wz7b",))

    def finalize(p):
        def act():
            for hm in range(4):
                unit = p * 4 + hm
                total = jnp.sum(l_st[unit], axis=0, keepdims=True)
                o_out[p - 1, hm * 128:(hm + 1) * 128, :] = (acc[unit] * (1.0 / total)).astype(BF16)
                st_out[p - 1, hm:hm + 1, :] = m_st[unit, 0:1, :]
                st_out[p - 1, 4 + hm:5 + hm, :] = total
            start(("o", p), ("st", p))
        return act

    phases = (
        (0, 2, (
            (got(("kd", 0), ("vd", 0)),),
            (got(("q", 2)), on("k", 1), lambda: start(("wz", 1), ("wz", 2)), w_across(0)),
            (got(("q", 3)), on("v", 1)),
            (got(("kd", 1), ("kd", 2)),),
        )),
        (2, 4, (
            (got(("vd", 1), ("vd", 2)), lambda: start(("s", 1), ("s", 3), ("s", 2))),
            (on("k", 3), w_on(0)),
            (w_ring(1), w_next(1)),
            (on("v", 3), got(("kd", 3), ("kd", 4))),
        )),
        (6, 4, (
            (got(("vd", 3), ("vd", 4)),),
            (w_last(0),),
            (on("k", 5),),
            (got(("kd", 5), ("kd", 6)), w_on(1)),
        )),
        (10, 4, (
            (on("v", 5), w_ring(3), got(("vd", 5), ("vd", 6))),
            (w_on(2),),
            (w_last(1), w_next(3)),
            (ring_end, got(("kd", 7))),
        )),
        (14, 2, (
            (got(("vd", 7)), w_on(3)),
            (finalize(3), w_last(2)),
            (finalize(2),),
            (finalize(1), w_on(4)),
        )),
    )

    def scores(s_buf, qi, hm, first, count):
        m, h = hm // 2, hm % 2
        q = q_all[qi, :, m * 128:(m + 1) * 128]
        lane = lax.broadcasted_iota(jnp.int32, q.shape, 1)
        q = jnp.where((lane >= 64) if h else (lane < 64), q, jnp.zeros_like(q))
        peak = None
        for b in range(count):
            s = lax.dot_general(
                k_all[first + b, :, m * 128:(m + 1) * 128], q, (((1,), (1,)), ((), ())),
                preferred_element_type=F32,
            )
            s_buf[b * 256:(b + 1) * 256, :] = s
            r = jnp.max(s.reshape(32, 8, 256), axis=0)
            peak = r if peak is None else jnp.maximum(peak, r)
        return peak

    def absorb(s_buf, unit, hm, first, count, peak):
        h = hm % 2
        m_old = m_st[unit]
        m_new = jnp.maximum(m_old, jnp.max(peak, axis=0, keepdims=True) * SCALE)
        rescale = jnp.exp2(m_old - m_new)
        m_st[unit] = m_new
        total, out = None, None
        for b in range(count):
            s = s_buf[b * 256:(b + 1) * 256, :].reshape(32, 8, 256)
            weights = jnp.exp2(s * SCALE - m_new[None])
            t = jnp.sum(weights, axis=0)
            total = t if total is None else total + t
            o = jnp.dot(
                v_all[first + b, h * 128:(h + 1) * 128, :], weights.reshape(256, 256).astype(BF16),
                preferred_element_type=F32,
            )
            out = o if out is None else out + o
        l_st[unit] = l_st[unit] * rescale + total
        acc[unit] = (acc[unit].reshape(16, 8, 256) * rescale[None] + out.reshape(16, 8, 256)).reshape(128, 256)

    bufs = (sb0, sb1)

    def visit(qi, first, count, peak, qi_ahead, first_ahead, count_ahead):
        for hm in range(4):
            if hm < 3:
                ahead = scores(bufs[(hm + 1) % 2], qi, hm + 1, first, count)
            else:
                ahead = scores(bufs[0], qi_ahead, 0, first_ahead, count_ahead)
            absorb(bufs[hm % 2], qi * 4 + hm, hm, first, count, peak)
            peak = ahead
        return peak

    peak = None
    for n, (first, count, actions) in enumerate(phases):
        closing = n == len(phases) - 1
        for action in actions[0]:
            action()
        if peak is None:
            peak = scores(bufs[0], 0, 0, first, count)
            visit(0, first, count, peak, 0, first, count)
            arrive(("q", 1))
            peak = scores(bufs[0], 1, 0, first, count)

        def body(i, peak):
            for at_step in (1, 2):
                if actions[at_step]:
                    @pl.when(i == at_step)
                    def _():
                        for action in actions[at_step]:
                            action()
            qi = 3 - i if closing else i
            return visit(qi, first, count, peak, qi - 1 if closing else qi + 1, first, count)

        peak = lax.fori_loop(0 if n else 1, 3, body, peak)
        for action in actions[3]:
            action()
        if closing:
            visit(0, first, count, peak, 0, first, count)
        else:
            ahead = phases[n + 1]
            opening = 3 if n + 2 == len(phases) else 0
            peak = visit(3, first, count, peak, opening, ahead[0], ahead[1])

    w_last(3)()
    w_ring(5)()
    w_next(5)()
    arrive(("o", 3), ("st", 3))
    arrive(("o", 2), ("st", 2))
    arrive(("o", 1), ("st", 1))
    for h in range(2):
        maps = []
        for m in range(2):
            hm = m * 2 + h
            unit = hm
            peaks = [st_in[p, hm:hm + 1, :] for p in range(3)] + [m_st[unit, 0:1, :]]
            sums = [st_in[p, 4 + hm:5 + hm, :] for p in range(3)] + [jnp.sum(l_st[unit], axis=0, keepdims=True)]
            top = functools.reduce(jnp.maximum, peaks)
            powers = [jnp.exp2(v - top) for v in peaks]
            total = sum(v * l for v, l in zip(powers, sums))
            inverse = 1.0 / total
            merged = acc[unit] * (powers[3] * inverse)
            for p in range(3):
                merged += o_in[p, hm * 128:(hm + 1) * 128, :].astype(F32) * (powers[p] * sums[p] * inverse)
            maps.append(merged)
        differ = maps[0] - lam_ref[h] * maps[1]
        mean_square = jnp.mean(differ * differ, axis=0, keepdims=True)
        scaled = jnp.transpose(differ * lax.rsqrt(mean_square + EPSILON))
        att[x, :, h * 128:(h + 1) * 128] = (scaled * hg_ref[...] * 0.8).astype(BF16)
    exchange = [("a", 2), ("a", 1), ("a", 3)]
    start(*exchange)
    w_ring_end()
    w_across(7)()
    w_last(4)()
    w_on(5)()
    w_on(6)()
    wo_copy.wait()
    arrive(*exchange)

    arrive(("s", 1), ("s", 2), ("s", 3))
    row_sums[...] = jnp.zeros_like(row_sums)

    def project(n, carry):
        cols = pl.ds(pl.multiple_of(n * 512, 512), 512)
        total = None
        for i in range(4):
            term = jnp.dot(att[i], wo_v[i * 256:(i + 1) * 256, cols], preferred_element_type=F32)
            total = term if total is None else total + term
        mixed = ALPHA * s_all[:, :, cols].reshape(256, 512).astype(F32) + total
        branch[:, cols] = mixed
        row_sums[...] += sum(mixed[:, i * 128:(i + 1) * 128] for i in range(4))
        return carry

    lax.fori_loop(0, 4, project, 0)
    w_last(5)()
    w_last(6)()
    w_on(7)()
    mean = jnp.sum(row_sums[...], axis=-1, keepdims=True) * (1.0 / 2048)
    row_sums[...] = jnp.broadcast_to(mean, (256, 128))
    spread = None
    for n in range(16):
        centered = branch[:, n * 128:(n + 1) * 128] - row_sums[...]
        spread = centered * centered if spread is None else spread + centered * centered
    var = jnp.sum(spread, axis=-1, keepdims=True) * (1.0 / 2048)
    inverse = jnp.broadcast_to(lax.rsqrt(var + EPSILON), (256, 128))
    for n in range(16):
        cols = slice(n * 128, (n + 1) * 128)
        normed[:, cols] = ((branch[:, cols] - row_sums[...]) * inverse * ng_ref[:, cols]).astype(BF16)
    w_last(7)()
    for kind in ("wd0", "wd1", "wd2", "wd3"):
        arrive(*[(kind, i) for i in range(8)])
    for lo, hi in ((0, 256), (256, 512), (512, 704)):
        gate = jnp.dot(normed[...], w_all[:, 0:32, lo:hi].reshape(2048, hi - lo), preferred_element_type=F32)
        upward = jnp.dot(normed[...], w_all[:, 32:64, lo:hi].reshape(2048, hi - lo), preferred_element_type=F32)
        hidden[:, lo:hi] = (gate / (1.0 + jnp.exp(-gate)) * upward).astype(BF16)
    for h in range(2):
        def down(n, carry):
            rows_of = pl.ds(pl.multiple_of((h * 4 + n) * 8, 8), 8)
            product = lax.dot_general(
                hidden[...], w_all[rows_of, 64:96, :].reshape(256, 704), (((1,), (1,)), ((), ())),
                preferred_element_type=F32,
            ).astype(BF16)
            cols = pl.ds(pl.multiple_of(n * 256, 256), 256)
            part[h, :, cols] = product
            return carry

        lax.fori_loop(0, 4, down, 0)
        start(("p", h, 2), ("p", h, 1), ("p", h, 3))
    own_rows = pl.ds(pl.multiple_of(x * 64, 64), 64)
    for h in range(2):
        for j in range(1, 4):
            arrive(("p", h, j))
        cols = slice(h * 1024, (h + 1) * 1024)
        mixer = part[h, own_rows, :].astype(F32)
        for j in range(1, 4):
            mixer += part_in[h, j].astype(F32)
        out_ref[:, cols] = (ALPHA * normed[own_rows, cols].astype(F32) + 0.5 * mixer).astype(BF16)
    for name in NAMES:
        describe(name).wait_send()


def on_device(
    stream, query_one, key_one, query_two, key_two, values, lambdas, head_gain, out_weight, norm_gain,
    gate_weight, up_weight, down_weight,
):
    whole = pl.BlockSpec(memory_space=pl.ANY)
    vmem = pl.BlockSpec(memory_space=pltpu.VMEM)
    return pl.pallas_call(
        kernel,
        out_shape=jax.ShapeDtypeStruct((64, 2048), BF16),
        in_specs=[whole] * 9 + [pl.BlockSpec(memory_space=pltpu.SMEM), vmem, vmem, whole],
        out_specs=vmem,
        scratch_shapes=[
            pltpu.VMEM((4, 256, 256), BF16),
            pltpu.VMEM((16, 256, 256), BF16),
            pltpu.VMEM((16, 256, 256), BF16),
            pltpu.VMEM((256, 256), BF16),
            pltpu.VMEM((16, 128, 256), F32),
            pltpu.VMEM((16, 8, 256), F32),
            pltpu.VMEM((16, 8, 256), F32),
            pltpu.VMEM((1024, 256), F32),
            pltpu.VMEM((1024, 256), F32),
            pltpu.VMEM((64, 96, 704), BF16),
            pltpu.VMEM((4, 64, 2048), BF16),
            pltpu.VMEM((1024, 2048), BF16),
            pltpu.VMEM((3, 512, 256), BF16),
            pltpu.VMEM((3, 8, 256), F32),
            pltpu.VMEM((3, 512, 256), BF16),
            pltpu.VMEM((3, 8, 256), F32),
            pltpu.VMEM((4, 256, 256), BF16),
            pltpu.VMEM((256, 2048), F32),
            pltpu.VMEM((256, 128), F32),
            pltpu.VMEM((256, 2048), BF16),
            pltpu.VMEM((256, 704), BF16),
            pltpu.VMEM((2, 256, 1024), BF16),
            pltpu.VMEM((2, 4, 64, 1024), BF16),
            pltpu.SemaphoreType.DMA((len(NAMES),)),
            pltpu.SemaphoreType.DMA((len(NAMES),)),
            pltpu.SemaphoreType.DMA((12,)),
        ],
        compiler_params=pltpu.CompilerParams(
            collective_id=0, has_side_effects=True, vmem_limit_bytes=60 * 2**20
        ),
    )(
        query_one, query_two, key_one, key_two, values, gate_weight, up_weight, jnp.transpose(down_weight), stream, lambdas, head_gain.reshape(1, 128), norm_gain.reshape(1, 2048),
        out_weight,
    )


def solution(mesh):
    return jax.shard_map(
        on_device,
        mesh=mesh,
        in_specs=(
            P(("sp", "tp"), None), P("sp", "tp"), P("sp", "tp"), P("sp", "tp"), P("sp", "tp"), P("sp", "tp"),
            P("tp"), P(), P(), P(), P("sp", "tp"), P("sp", "tp"), P("tp", "sp"),
        ),
        out_specs=P(("sp", "tp"), None),
        check_vma=False,
    )
```

```python
import functools
import math

import jax
import jax.numpy as jnp
from jax import lax
from jax.experimental import pallas as pl
from jax.experimental.pallas import tpu as pltpu
from jax.sharding import PartitionSpec as P

MESH = pl.DeviceIdType.MESH
F32 = jnp.float32
BF16 = jnp.bfloat16
ALPHA = 1.4142135623730951
EPSILON = 1e-05
SCALE = math.log2(math.e) / 8.0
REL = (0, 1, 3, 2)
Z_OF_SLOT = (0, -1, 1, -2, 2, -3, 3, 4)


def message_names():
    names = [("q", p) for p in range(1, 4)]
    for a in "kv":
        names += [(a, s) for s in range(1, 8)] + [(a + "d", s) for s in range(8)]
    names += [("wz", s) for s in range(1, 7)] + [("wz7a",), ("wz7b",)]
    for kind in ("wxl", "wxr", "wxa", "wxb", "wd0", "wd1", "wd2", "wd3"):
        names += [(kind, i) for i in range(8)]
    names += [(kind,) for kind in ("dyl", "dyr", "dya", "dyb", "dz7a", "dz7b")]
    names += [("dz", s) for s in range(1, 7)] + [("dd", i) for i in range(8)]
    names += [("s", j) for j in range(1, 4)]
    names += [("o", p) for p in range(1, 4)] + [("st", p) for p in range(1, 4)]
    names += [("a", j) for j in range(1, 4)]
    names += [("p", h, j) for h in range(2) for j in range(1, 4)]
    return names


NAMES = message_names()
INDEX = {name: i for i, name in enumerate(NAMES)}


def kernel(
    q1_ref, q2_ref, k1_ref, k2_ref, v_ref, g_ref, u_ref, d_ref, s_ref, lam_ref, hg_ref, ng_ref, wo_ref,
    out_ref,
    q_all, k_all, v_all, v_own, acc, m_st, l_st, sb0, sb1, w_all, d_all, s_all, wo_v,
    o_out, st_out, o_in, st_in, att, branch, row_sums, normed, hidden, part, part_in,
    send_sems, recv_sems, local_sems,
):
    sp = lax.axis_index("sp")
    x = lax.axis_index("tp")
    z = sp // 8
    y = lax.rem(sp, 8) // 2
    c = lax.rem(sp, 2)

    def mod(a, n):
        return lax.rem(a + 2 * n, n)

    def at(dz=0, dy=0, dc=0, dx=0):
        return {
            "sp": mod(z + dz, 8) * 8 + mod(y + dy, 4) * 2 + mod(c + dc, 2),
            "tp": mod(x + dx, 4),
        }

    def block(dz=0, dy=0):
        return mod(z + dz, 8) * 8 + mod(y + dy, 4) * 2 + c

    def remote(name, src, dst, target):
        i = INDEX[name]
        return pltpu.make_async_remote_copy(
            src_ref=src, dst_ref=dst, send_sem=send_sems.at[i], recv_sem=recv_sems.at[i],
            device_id=target, device_id_type=MESH,
        )

    def describe(name):
        kind = name[0]
        if kind == "q":
            p = name[1]
            return remote(name, q_all.at[0], q_all.at[p], at(dy=REL[p]))
        if kind in ("k", "v"):
            s = name[1]
            buf = k_all if kind == "k" else v_all
            step = 1 if s in (1, 3, 5) else -1
            before = s - 2
            if s == 7:
                step, before = (1, 5) if kind == "k" else (-1, 6)
            return remote(name, buf.at[2 * max(before, 0)], buf.at[2 * s], at(dz=step))
        if kind in ("kd", "vd"):
            s = name[1]
            buf = k_all if kind == "kd" else v_all
            return remote(name, buf.at[2 * s], buf.at[2 * s + 1], at(dc=1))
        if kind == "wz":
            s = name[1]
            step = 1 if s in (1, 3, 5) else -1
            ref = w_all.at[block(dz=Z_OF_SLOT[s - 2] if s > 2 else 0)]
            return remote(name, ref, ref, at(dz=step))
        if kind == "wz7a":
            ref = w_all.at[block(dz=-3), 0:32]
            return remote(name, ref, ref, at(dz=1))
        if kind == "wz7b":
            ref = w_all.at[block(dz=3), 32:64]
            return remote(name, ref, ref, at(dz=-1))
        if kind in ("wxl", "wxr"):
            ref = w_all.at[block(dz=Z_OF_SLOT[name[1]])]
            return remote(name, ref, ref, at(dy=1 if kind == "wxl" else -1))
        if kind == "wxa":
            ref = w_all.at[block(dz=Z_OF_SLOT[name[1]], dy=-1), 0:32]
            return remote(name, ref, ref, at(dy=1))
        if kind == "wxb":
            ref = w_all.at[block(dz=Z_OF_SLOT[name[1]], dy=1), 32:64]
            return remote(name, ref, ref, at(dy=-1))
        if kind[:2] == "wd":
            ref = w_all.at[block(dz=Z_OF_SLOT[name[1]], dy=(0, -1, 1, 2)[int(kind[2])])]
            return remote(name, ref, ref, at(dc=1))
        if kind in ("dyl", "dyr"):
            ref = d_all.at[z, c, y]
            return remote(name, ref, ref, at(dy=1 if kind == "dyl" else -1))
        if kind == "dya":
            ref = d_all.at[z, c, mod(y - 1, 4), 0:16]
            return remote(name, ref, ref, at(dy=1))
        if kind == "dyb":
            ref = d_all.at[z, c, mod(y + 1, 4), 16:32]
            return remote(name, ref, ref, at(dy=-1))
        if kind == "dz":
            s = name[1]
            ref = d_all.at[mod(z + (Z_OF_SLOT[s - 2] if s > 2 else 0), 8), c]
            return remote(name, ref, ref, at(dz=1 if s in (1, 3, 5) else -1))
        if kind == "dz7a":
            ref = d_all.at[mod(z - 3, 8), c, 0:2]
            return remote(name, ref, ref, at(dz=1))
        if kind == "dz7b":
            ref = d_all.at[mod(z + 3, 8), c, 2:4]
            return remote(name, ref, ref, at(dz=-1))
        if kind == "dd":
            ref = d_all.at[mod(z + Z_OF_SLOT[name[1]], 8), c]
            return remote(name, ref, ref, at(dc=1))
        if kind == "s":
            return remote(name, s_all.at[x], s_all.at[x], at(dx=name[1]))
        if kind == "o":
            p = name[1]
            return remote(name, o_out.at[p - 1], o_in.at[p - 1], at(dy=-REL[p]))
        if kind == "st":
            p = name[1]
            return remote(name, st_out.at[p - 1], st_in.at[p - 1], at(dy=-REL[p]))
        if kind == "a":
            return remote(name, att.at[x], att.at[x], at(dx=name[1]))
        if kind == "p":
            h, j = name[1:]
            rows = pl.multiple_of(mod(x - j, 4) * 64, 64)
            return remote(name, part.at[h, pl.ds(rows, 64)], part_in.at[h, j], at(dx=-j))
        raise KeyError(kind)

    def start(*names):
        for name in names:
            describe(name).start()

    def arrive(*names):
        for name in names:
            describe(name).wait_recv()

    barrier = pltpu.get_barrier_semaphore()
    partners = [at(dz=1), at(dz=-1), at(dc=1)]
    partners += [at(dy=j) for j in range(1, 4)] + [at(dx=j) for j in range(1, 4)]
    for partner in partners:
        pl.semaphore_signal(barrier, inc=1, device_id=partner, device_id_type=MESH)
    takes = [
        pltpu.make_async_copy(src, dst, local_sems.at[3 + i])
        for i, (src, dst) in enumerate((
            (v_ref, v_own), (q1_ref, q_all.at[0, :, 0:128]), (q2_ref, q_all.at[0, :, 128:256]),
            (k1_ref, k_all.at[0, :, 0:128]), (k2_ref, k_all.at[0, :, 128:256]),
            (g_ref, w_all.at[sp, 0:32]), (u_ref, w_all.at[sp, 32:64]), (d_ref, d_all.at[z, c, y]), (s_ref, s_all.at[x]),
        ))
    ]
    for take in takes:
        take.start()
    wo_copy = pltpu.make_async_copy(wo_ref, wo_v, local_sems.at[0])
    wo_copy.start()
    m_st[...] = jnp.full_like(m_st, -1e30)
    l_st[...] = jnp.zeros_like(l_st)
    acc[...] = jnp.zeros_like(acc)
    takes[0].wait()
    v_all[0] = jnp.transpose(v_own[...])
    for take in takes[1:]:
        take.wait()
    pl.semaphore_wait(barrier, len(partners))

    start(("q", 1), ("q", 2), ("kd", 0), ("k", 1), ("k", 2), ("vd", 0), ("v", 1), ("v", 2), ("q", 3))

    def w_across(i):
        def act():
            start(("wxl", i), ("wxr", i), ("wd0", i))
        return act

    def w_on(i):
        def act():
            arrive(("wxl", i), ("wxr", i))
            start(("wxa", i), ("wxb", i), ("wd1", i), ("wd2", i))
        return act

    def w_last(i):
        def act():
            arrive(("wxa", i), ("wxb", i))
            start(("wd3", i))
        return act

    def on(a, s):
        def act():
            arrive((a, s), (a, s + 1))
            if s < 5:
                start((a, s + 2), (a, s + 3))
            else:
                start((a, 7))
            start((a + "d", s), (a + "d", s + 1))
        return act

    def ring_end():
        arrive(("k", 7), ("v", 7))
        start(("kd", 7), ("vd", 7))

    def got(*names):
        return lambda: arrive(*names)

    def w_ring(s):
        def act():
            arrive(("wz", s), ("wz", s + 1))
            w_across(s)()
            w_across(s + 1)()
        return act

    def w_next(s):
        def act():
            if s < 5:
                start(("wz", s + 2), ("wz", s + 3))
            else:
                start(("wz7a",), ("wz7b",))
        return act

    def w_ring_end():
        arrive(("wz7a",), ("wz7b",))

    def finalize(p):
        def act():
            for hm in range(4):
                unit = p * 4 + hm
                total = jnp.sum(l_st[unit], axis=0, keepdims=True)
                o_out[p - 1, hm * 128:(hm + 1) * 128, :] = (acc[unit] * (1.0 / total)).astype(BF16)
                st_out[p - 1, hm:hm + 1, :] = m_st[unit, 0:1, :]
                st_out[p - 1, 4 + hm:5 + hm, :] = total
            start(("o", p), ("st", p))
        return act

    def d_first():
        start(("dyl",), ("dyr",))

    def d_on():
        arrive(("dyl",), ("dyr",))
        start(("dya",), ("dyb",))

    def d_last():
        arrive(("dya",), ("dyb",))
        start(("dd", 0))

    def d_ring(s):
        def act():
            arrive(("dz", s), ("dz", s + 1))
            if s < 5:
                start(("dz", s + 2), ("dz", s + 3))
            else:
                start(("dz7a",), ("dz7b",))
            start(("dd", s), ("dd", s + 1))
        return act

    phases = (
        (0, 2, (
            (got(("kd", 0), ("vd", 0)),),
            (got(("q", 2)), on("k", 1), lambda: start(("wz", 1), ("wz", 2)), w_across(0), d_first),
            (got(("q", 3)), on("v", 1)),
            (got(("kd", 1), ("kd", 2)),),
        )),
        (2, 4, (
            (got(("vd", 1), ("vd", 2)), lambda: start(("s", 1), ("s", 3), ("s", 2))),
            (on("k", 3), w_on(0), d_on),
            (w_ring(1), w_next(1)),
            (on("v", 3), got(("kd", 3), ("kd", 4))),
        )),
        (6, 4, (
            (got(("vd", 3), ("vd", 4)),),
            (w_last(0), d_last),
            (on("k", 5),),
            (got(("kd", 5), ("kd", 6)), w_on(1)),
        )),
        (10, 4, (
            (on("v", 5), w_ring(3), w_next(3), lambda: start(("dz", 1), ("dz", 2)), got(("vd", 5), ("vd", 6))),
            (w_on(2),),
            (w_last(1), w_on(3)),
            (ring_end, got(("kd", 7))),
        )),
        (14, 2, (
            (got(("vd", 7)),),
            (finalize(3), w_on(4), w_last(2)),
            (finalize(2),),
            (finalize(1), w_ring(5), w_next(5)),
        )),
    )

    def scores(s_buf, qi, hm, first, count):
        m, h = hm // 2, hm % 2
        q = q_all[qi, :, m * 128:(m + 1) * 128]
        lane = lax.broadcasted_iota(jnp.int32, q.shape, 1)
        q = jnp.where((lane >= 64) if h else (lane < 64), q, jnp.zeros_like(q))
        peak = None
        for b in range(count):
            s = lax.dot_general(
                k_all[first + b, :, m * 128:(m + 1) * 128], q, (((1,), (1,)), ((), ())),
                preferred_element_type=F32,
            )
            s_buf[b * 256:(b + 1) * 256, :] = s
            r = jnp.max(s.reshape(32, 8, 256), axis=0)
            peak = r if peak is None else jnp.maximum(peak, r)
        return peak

    def absorb(s_buf, unit, hm, first, count, peak):
        h = hm % 2
        m_old = m_st[unit]
        m_new = jnp.maximum(m_old, jnp.max(peak, axis=0, keepdims=True) * SCALE)
        rescale = jnp.exp2(m_old - m_new)
        m_st[unit] = m_new
        total, out = None, None
        for b in range(count):
            s = s_buf[b * 256:(b + 1) * 256, :].reshape(32, 8, 256)
            weights = jnp.exp2(s * SCALE - m_new[None])
            t = jnp.sum(weights, axis=0)
            total = t if total is None else total + t
            o = jnp.dot(
                v_all[first + b, h * 128:(h + 1) * 128, :], weights.reshape(256, 256).astype(BF16),
                preferred_element_type=F32,
            )
            out = o if out is None else out + o
        l_st[unit] = l_st[unit] * rescale + total
        acc[unit] = (acc[unit].reshape(16, 8, 256) * rescale[None] + out.reshape(16, 8, 256)).reshape(128, 256)

    bufs = (sb0, sb1)

    def visit(qi, first, count, peak, qi_ahead, first_ahead, count_ahead):
        for hm in range(4):
            if hm < 3:
                ahead = scores(bufs[(hm + 1) % 2], qi, hm + 1, first, count)
            else:
                ahead = scores(bufs[0], qi_ahead, 0, first_ahead, count_ahead)
            absorb(bufs[hm % 2], qi * 4 + hm, hm, first, count, peak)
            peak = ahead
        return peak

    peak = None
    for n, (first, count, actions) in enumerate(phases):
        closing = n == len(phases) - 1
        for action in actions[0]:
            action()
        if peak is None:
            peak = scores(bufs[0], 0, 0, first, count)
            visit(0, first, count, peak, 0, first, count)
            arrive(("q", 1))
            peak = scores(bufs[0], 1, 0, first, count)

        def body(i, peak):
            for at_step in (1, 2):
                if actions[at_step]:
                    @pl.when(i == at_step)
                    def _():
                        for action in actions[at_step]:
                            action()
            qi = 3 - i if closing else i
            return visit(qi, first, count, peak, qi - 1 if closing else qi + 1, first, count)

        peak = lax.fori_loop(0 if n else 1, 3, body, peak)
        for action in actions[3]:
            action()
        if closing:
            visit(0, first, count, peak, 0, first, count)
        else:
            ahead = phases[n + 1]
            opening = 3 if n + 2 == len(phases) else 0
            peak = visit(3, first, count, peak, opening, ahead[0], ahead[1])

    w_last(3)()
    d_ring(1)()
    arrive(("o", 3), ("st", 3))
    w_ring_end()
    w_across(7)()
    arrive(("o", 2), ("st", 2))
    arrive(("o", 1), ("st", 1))
    for h in range(2):
        maps = []
        for m in range(2):
            hm = m * 2 + h
            unit = hm
            peaks = [st_in[p, hm:hm + 1, :] for p in range(3)] + [m_st[unit, 0:1, :]]
            sums = [st_in[p, 4 + hm:5 + hm, :] for p in range(3)] + [jnp.sum(l_st[unit], axis=0, keepdims=True)]
            top = functools.reduce(jnp.maximum, peaks)
            powers = [jnp.exp2(v - top) for v in peaks]
            total = sum(v * l for v, l in zip(powers, sums))
            inverse = 1.0 / total
            merged = acc[unit] * (powers[3] * inverse)
            for p in range(3):
                merged += o_in[p, hm * 128:(hm + 1) * 128, :].astype(F32) * (powers[p] * sums[p] * inverse)
            maps.append(merged)
        differ = maps[0] - lam_ref[h] * maps[1]
        mean_square = jnp.mean(differ * differ, axis=0, keepdims=True)
        scaled = jnp.transpose(differ * lax.rsqrt(mean_square + EPSILON))
        att[x, :, h * 128:(h + 1) * 128] = (scaled * hg_ref[...] * 0.8).astype(BF16)
    exchange = [("a", 2), ("a", 1), ("a", 3)]
    start(*exchange)
    w_last(4)()
    w_on(5)()
    w_on(6)()
    d_ring(3)()
    w_on(7)()
    wo_copy.wait()
    arrive(*exchange)

    arrive(("s", 1), ("s", 2), ("s", 3))
    row_sums[...] = jnp.zeros_like(row_sums)

    def project(n, carry):
        cols = pl.ds(pl.multiple_of(n * 512, 512), 512)
        total = None
        for i in range(4):
            term = jnp.dot(att[i], wo_v[i * 256:(i + 1) * 256, cols], preferred_element_type=F32)
            total = term if total is None else total + term
        mixed = ALPHA * s_all[:, :, cols].reshape(256, 512).astype(F32) + total
        branch[:, cols] = mixed
        row_sums[...] += sum(mixed[:, i * 128:(i + 1) * 128] for i in range(4))
        return carry

    lax.fori_loop(0, 4, project, 0)
    w_last(5)()
    w_last(6)()
    d_ring(5)()
    mean = jnp.sum(row_sums[...], axis=-1, keepdims=True) * (1.0 / 2048)
    row_sums[...] = jnp.broadcast_to(mean, (256, 128))
    spread = None
    for n in range(16):
        centered = branch[:, n * 128:(n + 1) * 128] - row_sums[...]
        spread = centered * centered if spread is None else spread + centered * centered
    var = jnp.sum(spread, axis=-1, keepdims=True) * (1.0 / 2048)
    inverse = jnp.broadcast_to(lax.rsqrt(var + EPSILON), (256, 128))
    for n in range(16):
        cols = slice(n * 128, (n + 1) * 128)
        normed[:, cols] = ((branch[:, cols] - row_sums[...]) * inverse * ng_ref[:, cols]).astype(BF16)
    w_last(7)()
    arrive(("dz7a",), ("dz7b",))
    start(("dd", 7))
    for kind in ("wd0", "wd1", "wd2", "wd3"):
        arrive(*[(kind, i) for i in range(8)])
    for lo, hi in ((0, 256), (256, 512), (512, 704)):
        gate = jnp.dot(normed[...], w_all[:, 0:32, lo:hi].reshape(2048, hi - lo), preferred_element_type=F32)
        upward = jnp.dot(normed[...], w_all[:, 32:64, lo:hi].reshape(2048, hi - lo), preferred_element_type=F32)
        hidden[:, lo:hi] = (gate / (1.0 + jnp.exp(-gate)) * upward).astype(BF16)
    arrive(*[("dd", i) for i in range(8)])
    for h in range(2):
        def down(n, carry):
            columns = jnp.concatenate([d_all[h * 4 + n, i % 2, i // 2] for i in range(8)], axis=0)
            product = lax.dot_general(
                hidden[...], columns, (((1,), (1,)), ((), ())),
                preferred_element_type=F32,
            ).astype(BF16)
            cols = pl.ds(pl.multiple_of(n * 256, 256), 256)
            part[h, :, cols] = product
            return carry

        lax.fori_loop(0, 4, down, 0)
        start(("p", h, 2), ("p", h, 1), ("p", h, 3))
    own_rows = pl.ds(pl.multiple_of(x * 64, 64), 64)
    for h in range(2):
        for j in range(1, 4):
            arrive(("p", h, j))
        cols = slice(h * 1024, (h + 1) * 1024)
        mixer = part[h, own_rows, :].astype(F32)
        for j in range(1, 4):
            mixer += part_in[h, j].astype(F32)
        out_ref[:, cols] = (ALPHA * normed[own_rows, cols].astype(F32) + 0.5 * mixer).astype(BF16)
    for name in NAMES:
        describe(name).wait_send()


def on_device(
    stream, query_one, key_one, query_two, key_two, values, lambdas, head_gain, out_weight, norm_gain,
    gate_weight, up_weight, down_weight,
):
    whole = pl.BlockSpec(memory_space=pl.ANY)
    vmem = pl.BlockSpec(memory_space=pltpu.VMEM)
    return pl.pallas_call(
        kernel,
        out_shape=jax.ShapeDtypeStruct((64, 2048), BF16),
        in_specs=[whole] * 9 + [pl.BlockSpec(memory_space=pltpu.SMEM), vmem, vmem, whole],
        out_specs=vmem,
        scratch_shapes=[
            pltpu.VMEM((4, 256, 256), BF16),
            pltpu.VMEM((16, 256, 256), BF16),
            pltpu.VMEM((16, 256, 256), BF16),
            pltpu.VMEM((256, 256), BF16),
            pltpu.VMEM((16, 128, 256), F32),
            pltpu.VMEM((16, 8, 256), F32),
            pltpu.VMEM((16, 8, 256), F32),
            pltpu.VMEM((1024, 256), F32),
            pltpu.VMEM((1024, 256), F32),
            pltpu.VMEM((64, 64, 704), BF16),
            pltpu.VMEM((8, 2, 4, 32, 704), BF16),
            pltpu.VMEM((4, 64, 2048), BF16),
            pltpu.VMEM((1024, 2048), BF16),
            pltpu.VMEM((3, 512, 256), BF16),
            pltpu.VMEM((3, 8, 256), F32),
            pltpu.VMEM((3, 512, 256), BF16),
            pltpu.VMEM((3, 8, 256), F32),
            pltpu.VMEM((4, 256, 256), BF16),
            pltpu.VMEM((256, 2048), F32),
            pltpu.VMEM((256, 128), F32),
            pltpu.VMEM((256, 2048), BF16),
            pltpu.VMEM((256, 704), BF16),
            pltpu.VMEM((2, 256, 1024), BF16),
            pltpu.VMEM((2, 4, 64, 1024), BF16),
            pltpu.SemaphoreType.DMA((len(NAMES),)),
            pltpu.SemaphoreType.DMA((len(NAMES),)),
            pltpu.SemaphoreType.DMA((12,)),
        ],
        compiler_params=pltpu.CompilerParams(
            collective_id=0, has_side_effects=True, vmem_limit_bytes=60 * 2**20
        ),
    )(
        query_one, query_two, key_one, key_two, values, gate_weight, up_weight, jnp.transpose(down_weight), stream, lambdas, head_gain.reshape(1, 128), norm_gain.reshape(1, 2048),
        out_weight,
    )


def solution(mesh):
    return jax.shard_map(
        on_device,
        mesh=mesh,
        in_specs=(
            P(("sp", "tp"), None), P("sp", "tp"), P("sp", "tp"), P("sp", "tp"), P("sp", "tp"), P("sp", "tp"),
            P("tp"), P(), P(), P(), P("sp", "tp"), P("sp", "tp"), P("tp", "sp"),
        ),
        out_specs=P(("sp", "tp"), None),
        check_vma=False,
    )
```

```python
import functools
import math

import jax
import jax.numpy as jnp
from jax import lax
from jax.experimental import pallas as pl
from jax.experimental.pallas import tpu as pltpu
from jax.sharding import PartitionSpec as P

MESH = pl.DeviceIdType.MESH
F32 = jnp.float32
BF16 = jnp.bfloat16
ALPHA = 1.4142135623730951
EPSILON = 1e-05
SCALE = math.log2(math.e) / 8.0
REL = (0, 1, 3, 2)
Z_OF_SLOT = (0, -1, 1, -2, 2, -3, 3, 4)


def message_names():
    names = [("q", p) for p in range(1, 4)]
    for a in "kv":
        names += [(a, s) for s in range(1, 8)] + [(a + "d", s) for s in range(8)]
    names += [("wz", s) for s in range(1, 7)] + [("wz7a",), ("wz7b",)]
    for kind in ("wxl", "wxr", "wxa", "wxb", "wd0", "wd1", "wd2", "wd3"):
        names += [(kind, i) for i in range(8)]
    names += [(kind,) for kind in ("dyl", "dyr", "dya", "dyb", "dz7a", "dz7b")]
    names += [("dz", s) for s in range(1, 7)] + [("dd", i) for i in range(8)]
    names += [("s", j) for j in range(1, 4)]
    names += [("o", p) for p in range(1, 4)] + [("st", p) for p in range(1, 4)]
    names += [("a", j) for j in range(1, 4)]
    names += [(kind, h) for kind in ("fa", "fb", "u1", "u3", "m1", "m3") for h in range(2)]
    return names


NAMES = message_names()
INDEX = {name: i for i, name in enumerate(NAMES)}


def kernel(
    q1_ref, q2_ref, k1_ref, k2_ref, v_ref, g_ref, u_ref, d_ref, s_ref, lam_ref, hg_ref, ng_ref, wo_ref,
    out_ref,
    q_all, k_all, v_all, v_own, acc, m_st, l_st, sb0, sb1, w_all, d_all, s_all, wo_v,
    o_out, st_out, o_in, st_in, att, branch, row_sums, normed, hidden, part, part_in, far_in, merged_out,
    send_sems, recv_sems, local_sems,
):
    sp = lax.axis_index("sp")
    x = lax.axis_index("tp")
    z = sp // 8
    y = lax.rem(sp, 8) // 2
    c = lax.rem(sp, 2)

    def mod(a, n):
        return lax.rem(a + 2 * n, n)

    def at(dz=0, dy=0, dc=0, dx=0):
        return {
            "sp": mod(z + dz, 8) * 8 + mod(y + dy, 4) * 2 + mod(c + dc, 2),
            "tp": mod(x + dx, 4),
        }

    def block(dz=0, dy=0):
        return mod(z + dz, 8) * 8 + mod(y + dy, 4) * 2 + c

    def partial_rows(j, offset):
        return pl.ds(pl.multiple_of(mod(x - j, 4) * 64 + offset, 32), 32)

    def remote(name, src, dst, target):
        i = INDEX[name]
        return pltpu.make_async_remote_copy(
            src_ref=src, dst_ref=dst, send_sem=send_sems.at[i], recv_sem=recv_sems.at[i],
            device_id=target, device_id_type=MESH,
        )

    def describe(name):
        kind = name[0]
        if kind == "q":
            p = name[1]
            return remote(name, q_all.at[0], q_all.at[p], at(dy=REL[p]))
        if kind in ("k", "v"):
            s = name[1]
            buf = k_all if kind == "k" else v_all
            step = 1 if s in (1, 3, 5) else -1
            before = s - 2
            if s == 7:
                step, before = (1, 5) if kind == "k" else (-1, 6)
            return remote(name, buf.at[2 * max(before, 0)], buf.at[2 * s], at(dz=step))
        if kind in ("kd", "vd"):
            s = name[1]
            buf = k_all if kind == "kd" else v_all
            return remote(name, buf.at[2 * s], buf.at[2 * s + 1], at(dc=1))
        if kind == "wz":
            s = name[1]
            step = 1 if s in (1, 3, 5) else -1
            ref = w_all.at[block(dz=Z_OF_SLOT[s - 2] if s > 2 else 0)]
            return remote(name, ref, ref, at(dz=step))
        if kind == "wz7a":
            ref = w_all.at[block(dz=-3), 0:32]
            return remote(name, ref, ref, at(dz=1))
        if kind == "wz7b":
            ref = w_all.at[block(dz=3), 32:64]
            return remote(name, ref, ref, at(dz=-1))
        if kind in ("wxl", "wxr"):
            ref = w_all.at[block(dz=Z_OF_SLOT[name[1]])]
            return remote(name, ref, ref, at(dy=1 if kind == "wxl" else -1))
        if kind == "wxa":
            ref = w_all.at[block(dz=Z_OF_SLOT[name[1]], dy=-1), 0:32]
            return remote(name, ref, ref, at(dy=1))
        if kind == "wxb":
            ref = w_all.at[block(dz=Z_OF_SLOT[name[1]], dy=1), 32:64]
            return remote(name, ref, ref, at(dy=-1))
        if kind[:2] == "wd":
            ref = w_all.at[block(dz=Z_OF_SLOT[name[1]], dy=(0, -1, 1, 2)[int(kind[2])])]
            return remote(name, ref, ref, at(dc=1))
        if kind in ("dyl", "dyr"):
            ref = d_all.at[z, c, y]
            return remote(name, ref, ref, at(dy=1 if kind == "dyl" else -1))
        if kind == "dya":
            ref = d_all.at[z, c, mod(y - 1, 4), 0:16]
            return remote(name, ref, ref, at(dy=1))
        if kind == "dyb":
            ref = d_all.at[z, c, mod(y + 1, 4), 16:32]
            return remote(name, ref, ref, at(dy=-1))
        if kind == "dz":
            s = name[1]
            ref = d_all.at[mod(z + (Z_OF_SLOT[s - 2] if s > 2 else 0), 8), c]
            return remote(name, ref, ref, at(dz=1 if s in (1, 3, 5) else -1))
        if kind == "dz7a":
            ref = d_all.at[mod(z - 3, 8), c, 0:2]
            return remote(name, ref, ref, at(dz=1))
        if kind == "dz7b":
            ref = d_all.at[mod(z + 3, 8), c, 2:4]
            return remote(name, ref, ref, at(dz=-1))
        if kind == "dd":
            ref = d_all.at[mod(z + Z_OF_SLOT[name[1]], 8), c]
            return remote(name, ref, ref, at(dc=1))
        if kind == "s":
            return remote(name, s_all.at[x], s_all.at[x], at(dx=name[1]))
        if kind == "o":
            p = name[1]
            return remote(name, o_out.at[p - 1], o_in.at[p - 1], at(dy=-REL[p]))
        if kind == "st":
            p = name[1]
            return remote(name, st_out.at[p - 1], st_in.at[p - 1], at(dy=-REL[p]))
        if kind == "a":
            return remote(name, att.at[x], att.at[x], at(dx=name[1]))
        h = name[1]
        if kind == "fa":
            return remote(name, part.at[h, partial_rows(2, 0)], far_in.at[h, 0], at(dx=-1))
        if kind == "fb":
            return remote(name, part.at[h, partial_rows(2, 32)], far_in.at[h, 1], at(dx=1))
        if kind == "u1":
            return remote(name, part.at[h, partial_rows(1, 32)], part_in.at[h, 0, 32:64], at(dx=-1))
        if kind == "u3":
            return remote(name, part.at[h, partial_rows(3, 0)], part_in.at[h, 1, 0:32], at(dx=1))
        if kind == "m1":
            return remote(name, merged_out.at[h, 0], part_in.at[h, 0, 0:32], at(dx=-1))
        if kind == "m3":
            return remote(name, merged_out.at[h, 1], part_in.at[h, 1, 32:64], at(dx=1))
        raise KeyError(kind)

    def start(*names):
        for name in names:
            describe(name).start()

    def arrive(*names):
        for name in names:
            describe(name).wait_recv()

    barrier = pltpu.get_barrier_semaphore()
    partners = [at(dz=1), at(dz=-1), at(dc=1)]
    partners += [at(dy=j) for j in range(1, 4)] + [at(dx=j) for j in range(1, 4)]
    for partner in partners:
        pl.semaphore_signal(barrier, inc=1, device_id=partner, device_id_type=MESH)
    takes = [
        pltpu.make_async_copy(src, dst, local_sems.at[3 + i])
        for i, (src, dst) in enumerate((
            (v_ref, v_own), (q1_ref, q_all.at[0, :, 0:128]), (q2_ref, q_all.at[0, :, 128:256]),
            (k1_ref, k_all.at[0, :, 0:128]), (k2_ref, k_all.at[0, :, 128:256]),
            (g_ref, w_all.at[sp, 0:32]), (u_ref, w_all.at[sp, 32:64]), (d_ref, d_all.at[z, c, y]), (s_ref, s_all.at[x]),
        ))
    ]
    for take in takes:
        take.start()
    wo_copy = pltpu.make_async_copy(wo_ref, wo_v, local_sems.at[0])
    wo_copy.start()
    m_st[...] = jnp.full_like(m_st, -1e30)
    l_st[...] = jnp.zeros_like(l_st)
    acc[...] = jnp.zeros_like(acc)
    takes[0].wait()
    v_all[0] = jnp.transpose(v_own[...])
    for take in takes[1:]:
        take.wait()
    pl.semaphore_wait(barrier, len(partners))

    start(("q", 1), ("q", 2), ("kd", 0), ("k", 1), ("k", 2), ("vd", 0), ("v", 1), ("v", 2), ("q", 3))

    def w_across(i):
        def act():
            start(("wxl", i), ("wxr", i), ("wd0", i))
        return act

    def w_on(i):
        def act():
            arrive(("wxl", i), ("wxr", i))
            start(("wxa", i), ("wxb", i), ("wd1", i), ("wd2", i))
        return act

    def w_last(i):
        def act():
            arrive(("wxa", i), ("wxb", i))
            start(("wd3", i))
        return act

    def on(a, s):
        def act():
            arrive((a, s), (a, s + 1))
            if s < 5:
                start((a, s + 2), (a, s + 3))
            else:
                start((a, 7))
            start((a + "d", s), (a + "d", s + 1))
        return act

    def ring_end():
        arrive(("k", 7), ("v", 7))
        start(("kd", 7), ("vd", 7))

    def got(*names):
        return lambda: arrive(*names)

    def w_ring(s):
        def act():
            arrive(("wz", s), ("wz", s + 1))
            w_across(s)()
            w_across(s + 1)()
        return act

    def w_next(s):
        def act():
            if s < 5:
                start(("wz", s + 2), ("wz", s + 3))
            else:
                start(("wz7a",), ("wz7b",))
        return act

    def w_ring_end():
        arrive(("wz7a",), ("wz7b",))

    def finalize(p):
        def act():
            for hm in range(4):
                unit = p * 4 + hm
                total = jnp.sum(l_st[unit], axis=0, keepdims=True)
                o_out[p - 1, hm * 128:(hm + 1) * 128, :] = (acc[unit] * (1.0 / total)).astype(BF16)
                st_out[p - 1, hm:hm + 1, :] = m_st[unit, 0:1, :]
                st_out[p - 1, 4 + hm:5 + hm, :] = total
            start(("o", p), ("st", p))
        return act

    def d_first():
        start(("dyl",), ("dyr",))

    def d_on():
        arrive(("dyl",), ("dyr",))
        start(("dya",), ("dyb",))

    def d_last():
        arrive(("dya",), ("dyb",))
        start(("dd", 0))

    def d_ring(s):
        def act():
            arrive(("dz", s), ("dz", s + 1))
            if s < 5:
                start(("dz", s + 2), ("dz", s + 3))
            else:
                start(("dz7a",), ("dz7b",))
            start(("dd", s), ("dd", s + 1))
        return act

    phases = (
        (0, 2, (
            (got(("kd", 0), ("vd", 0)),),
            (got(("q", 2)), on("k", 1), lambda: start(("wz", 1), ("wz", 2)), w_across(0), d_first),
            (got(("q", 3)), on("v", 1)),
            (got(("kd", 1), ("kd", 2)),),
        )),
        (2, 4, (
            (got(("vd", 1), ("vd", 2)), lambda: start(("s", 1), ("s", 3), ("s", 2))),
            (on("k", 3), w_on(0), d_on),
            (w_ring(1), w_next(1)),
            (on("v", 3), got(("kd", 3), ("kd", 4))),
        )),
        (6, 4, (
            (got(("vd", 3), ("vd", 4)),),
            (w_last(0), d_last),
            (on("k", 5),),
            (got(("kd", 5), ("kd", 6)), w_on(1)),
        )),
        (10, 4, (
            (on("v", 5), w_ring(3), w_next(3), lambda: start(("dz", 1), ("dz", 2)), got(("vd", 5), ("vd", 6))),
            (w_on(2),),
            (w_last(1), w_on(3)),
            (ring_end, got(("kd", 7))),
        )),
        (14, 2, (
            (got(("vd", 7)),),
            (finalize(3), w_on(4), w_last(2)),
            (finalize(2),),
            (finalize(1), got(("wz", 5), ("wz", 6)), w_next(5)),
        )),
    )

    def scores(s_buf, qi, hm, first, count):
        m, h = hm // 2, hm % 2
        q = q_all[qi, :, m * 128:(m + 1) * 128]
        lane = lax.broadcasted_iota(jnp.int32, q.shape, 1)
        q = jnp.where((lane >= 64) if h else (lane < 64), q, jnp.zeros_like(q))
        peak = None
        for b in range(count):
            s = lax.dot_general(
                k_all[first + b, :, m * 128:(m + 1) * 128], q, (((1,), (1,)), ((), ())),
                preferred_element_type=F32,
            )
            s_buf[b * 256:(b + 1) * 256, :] = s
            r = jnp.max(s.reshape(32, 8, 256), axis=0)
            peak = r if peak is None else jnp.maximum(peak, r)
        return peak

    def absorb(s_buf, unit, hm, first, count, peak):
        h = hm % 2
        m_old = m_st[unit]
        m_new = jnp.maximum(m_old, jnp.max(peak, axis=0, keepdims=True) * SCALE)
        rescale = jnp.exp2(m_old - m_new)
        m_st[unit] = m_new
        total, out = None, None
        for b in range(count):
            s = s_buf[b * 256:(b + 1) * 256, :].reshape(32, 8, 256)
            weights = jnp.exp2(s * SCALE - m_new[None])
            t = jnp.sum(weights, axis=0)
            total = t if total is None else total + t
            o = jnp.dot(
                v_all[first + b, h * 128:(h + 1) * 128, :], weights.reshape(256, 256).astype(BF16),
                preferred_element_type=F32,
            )
            out = o if out is None else out + o
        l_st[unit] = l_st[unit] * rescale + total
        acc[unit] = (acc[unit].reshape(16, 8, 256) * rescale[None] + out.reshape(16, 8, 256)).reshape(128, 256)

    bufs = (sb0, sb1)

    def visit(qi, first, count, peak, qi_ahead, first_ahead, count_ahead):
        for hm in range(4):
            if hm < 3:
                ahead = scores(bufs[(hm + 1) % 2], qi, hm + 1, first, count)
            else:
                ahead = scores(bufs[0], qi_ahead, 0, first_ahead, count_ahead)
            absorb(bufs[hm % 2], qi * 4 + hm, hm, first, count, peak)
            peak = ahead
        return peak

    peak = None
    for n, (first, count, actions) in enumerate(phases):
        closing = n == len(phases) - 1
        for action in actions[0]:
            action()
        if peak is None:
            peak = scores(bufs[0], 0, 0, first, count)
            visit(0, first, count, peak, 0, first, count)
            arrive(("q", 1))
            peak = scores(bufs[0], 1, 0, first, count)

        def body(i, peak):
            for at_step in (1, 2):
                if actions[at_step]:
                    @pl.when(i == at_step)
                    def _():
                        for action in actions[at_step]:
                            action()
            qi = 3 - i if closing else i
            return visit(qi, first, count, peak, qi - 1 if closing else qi + 1, first, count)

        peak = lax.fori_loop(0 if n else 1, 3, body, peak)
        for action in actions[3]:
            action()
        if closing:
            visit(0, first, count, peak, 0, first, count)
        else:
            ahead = phases[n + 1]
            opening = 3 if n + 2 == len(phases) else 0
            peak = visit(3, first, count, peak, opening, ahead[0], ahead[1])

    w_last(3)()
    d_ring(1)()
    arrive(("o", 3), ("st", 3))
    w_across(5)()
    w_across(6)()
    w_ring_end()
    d_ring(3)()
    arrive(("o", 2), ("st", 2))
    arrive(("o", 1), ("st", 1))
    w_across(7)()
    for h in range(2):
        maps = []
        for m in range(2):
            hm = m * 2 + h
            unit = hm
            peaks = [st_in[p, hm:hm + 1, :] for p in range(3)] + [m_st[unit, 0:1, :]]
            sums = [st_in[p, 4 + hm:5 + hm, :] for p in range(3)] + [jnp.sum(l_st[unit], axis=0, keepdims=True)]
            top = functools.reduce(jnp.maximum, peaks)
            powers = [jnp.exp2(v - top) for v in peaks]
            total = sum(v * l for v, l in zip(powers, sums))
            inverse = 1.0 / total
            merged = acc[unit] * (powers[3] * inverse)
            for p in range(3):
                merged += o_in[p, hm * 128:(hm + 1) * 128, :].astype(F32) * (powers[p] * sums[p] * inverse)
            maps.append(merged)
        differ = maps[0] - lam_ref[h] * maps[1]
        mean_square = jnp.mean(differ * differ, axis=0, keepdims=True)
        scaled = jnp.transpose(differ * lax.rsqrt(mean_square + EPSILON))
        att[x, :, h * 128:(h + 1) * 128] = (scaled * hg_ref[...] * 0.8).astype(BF16)
    exchange = [("a", 2), ("a", 1), ("a", 3)]
    start(*exchange)
    w_last(4)()
    d_ring(5)()
    w_on(5)()
    w_on(6)()
    w_on(7)()
    wo_copy.wait()
    arrive(*exchange)

    arrive(("s", 1), ("s", 2), ("s", 3))
    row_sums[...] = jnp.zeros_like(row_sums)

    def project(n, carry):
        cols = pl.ds(pl.multiple_of(n * 512, 512), 512)
        total = None
        for i in range(4):
            term = jnp.dot(att[i], wo_v[i * 256:(i + 1) * 256, cols], preferred_element_type=F32)
            total = term if total is None else total + term
        mixed = ALPHA * s_all[:, :, cols].reshape(256, 512).astype(F32) + total
        branch[:, cols] = mixed
        row_sums[...] += sum(mixed[:, i * 128:(i + 1) * 128] for i in range(4))
        return carry

    lax.fori_loop(0, 4, project, 0)
    w_last(5)()
    w_last(6)()
    arrive(("dz7a",), ("dz7b",))
    start(("dd", 7))
    mean = jnp.sum(row_sums[...], axis=-1, keepdims=True) * (1.0 / 2048)
    row_sums[...] = jnp.broadcast_to(mean, (256, 128))
    spread = None
    for n in range(16):
        centered = branch[:, n * 128:(n + 1) * 128] - row_sums[...]
        spread = centered * centered if spread is None else spread + centered * centered
    var = jnp.sum(spread, axis=-1, keepdims=True) * (1.0 / 2048)
    inverse = jnp.broadcast_to(lax.rsqrt(var + EPSILON), (256, 128))
    for n in range(16):
        cols = slice(n * 128, (n + 1) * 128)
        normed[:, cols] = ((branch[:, cols] - row_sums[...]) * inverse * ng_ref[:, cols]).astype(BF16)
    w_last(7)()
    for kind in ("wd0", "wd1", "wd2", "wd3"):
        arrive(*[(kind, i) for i in range(8)])
    for lo, hi in ((0, 256), (256, 512), (512, 704)):
        gate = jnp.dot(normed[...], w_all[:, 0:32, lo:hi].reshape(2048, hi - lo), preferred_element_type=F32)
        upward = jnp.dot(normed[...], w_all[:, 32:64, lo:hi].reshape(2048, hi - lo), preferred_element_type=F32)
        hidden[:, lo:hi] = (gate / (1.0 + jnp.exp(-gate)) * upward).astype(BF16)
    arrive(*[("dd", i) for i in range(8)])
    for h in range(2):
        def down(n, carry):
            columns = jnp.concatenate([d_all[h * 4 + n, i % 2, i // 2] for i in range(8)], axis=0)
            product = lax.dot_general(
                hidden[...], columns, (((1,), (1,)), ((), ())),
                preferred_element_type=F32,
            ).astype(BF16)
            cols = pl.ds(pl.multiple_of(n * 256, 256), 256)
            part[h, :, cols] = product
            return carry

        lax.fori_loop(0, 4, down, 0)
        start(("fa", h), ("fb", h), ("u1", h), ("u3", h))
    for h in range(2):
        arrive(("fa", h), ("fb", h))
        for side, (j, offset) in enumerate(((1, 0), (3, 32))):
            own = part[h, partial_rows(j, offset), :].astype(F32)
            merged_out[h, side] = (own + far_in[h, side].astype(F32)).astype(BF16)
        start(("m1", h), ("m3", h))
    own_rows = pl.ds(pl.multiple_of(x * 64, 64), 64)
    for h in range(2):
        arrive(("u1", h), ("u3", h), ("m1", h), ("m3", h))
        cols = slice(h * 1024, (h + 1) * 1024)
        mixer = part[h, own_rows, :].astype(F32)
        for side in range(2):
            mixer += part_in[h, side].astype(F32)
        out_ref[:, cols] = (ALPHA * normed[own_rows, cols].astype(F32) + 0.5 * mixer).astype(BF16)
    for name in NAMES:
        describe(name).wait_send()


def on_device(
    stream, query_one, key_one, query_two, key_two, values, lambdas, head_gain, out_weight, norm_gain,
    gate_weight, up_weight, down_weight,
):
    whole = pl.BlockSpec(memory_space=pl.ANY)
    vmem = pl.BlockSpec(memory_space=pltpu.VMEM)
    return pl.pallas_call(
        kernel,
        out_shape=jax.ShapeDtypeStruct((64, 2048), BF16),
        in_specs=[whole] * 9 + [pl.BlockSpec(memory_space=pltpu.SMEM), vmem, vmem, whole],
        out_specs=vmem,
        scratch_shapes=[
            pltpu.VMEM((4, 256, 256), BF16),
            pltpu.VMEM((16, 256, 256), BF16),
            pltpu.VMEM((16, 256, 256), BF16),
            pltpu.VMEM((256, 256), BF16),
            pltpu.VMEM((16, 128, 256), F32),
            pltpu.VMEM((16, 8, 256), F32),
            pltpu.VMEM((16, 8, 256), F32),
            pltpu.VMEM((1024, 256), F32),
            pltpu.VMEM((1024, 256), F32),
            pltpu.VMEM((64, 64, 704), BF16),
            pltpu.VMEM((8, 2, 4, 32, 704), BF16),
            pltpu.VMEM((4, 64, 2048), BF16),
            pltpu.VMEM((1024, 2048), BF16),
            pltpu.VMEM((3, 512, 256), BF16),
            pltpu.VMEM((3, 8, 256), F32),
            pltpu.VMEM((3, 512, 256), BF16),
            pltpu.VMEM((3, 8, 256), F32),
            pltpu.VMEM((4, 256, 256), BF16),
            pltpu.VMEM((256, 2048), F32),
            pltpu.VMEM((256, 128), F32),
            pltpu.VMEM((256, 2048), BF16),
            pltpu.VMEM((256, 704), BF16),
            pltpu.VMEM((2, 256, 1024), BF16),
            pltpu.VMEM((2, 2, 64, 1024), BF16),
            pltpu.VMEM((2, 2, 32, 1024), BF16),
            pltpu.VMEM((2, 2, 32, 1024), BF16),
            pltpu.SemaphoreType.DMA((len(NAMES),)),
            pltpu.SemaphoreType.DMA((len(NAMES),)),
            pltpu.SemaphoreType.DMA((12,)),
        ],
        compiler_params=pltpu.CompilerParams(
            collective_id=0, has_side_effects=True, vmem_limit_bytes=60 * 2**20
        ),
    )(
        query_one, query_two, key_one, key_two, values, gate_weight, up_weight, jnp.transpose(down_weight), stream, lambdas, head_gain.reshape(1, 128), norm_gain.reshape(1, 2048),
        out_weight,
    )


def solution(mesh):
    return jax.shard_map(
        on_device,
        mesh=mesh,
        in_specs=(
            P(("sp", "tp"), None), P("sp", "tp"), P("sp", "tp"), P("sp", "tp"), P("sp", "tp"), P("sp", "tp"),
            P("tp"), P(), P(), P(), P("sp", "tp"), P("sp", "tp"), P("tp", "sp"),
        ),
        out_specs=P(("sp", "tp"), None),
        check_vma=False,
    )
```

```python
import functools
import math

import jax
import jax.numpy as jnp
from jax import lax
from jax.experimental import pallas as pl
from jax.experimental.pallas import tpu as pltpu
from jax.sharding import PartitionSpec as P

MESH = pl.DeviceIdType.MESH
F32 = jnp.float32
BF16 = jnp.bfloat16
ALPHA = 1.4142135623730951
EPSILON = 1e-05
SCALE = math.log2(math.e) / 8.0
REL = (0, 1, 3, 2)
Z_OF_SLOT = (0, -1, 1, -2, 2, -3, 3, 4)


def message_names():
    names = [("q", p) for p in range(1, 4)]
    for a in "kv":
        names += [(a, s) for s in range(1, 8)] + [(a + "d", s) for s in range(8)]
    names += [("wz", s) for s in range(1, 7)] + [("wz7a",), ("wz7b",)]
    for kind in ("wxl", "wxr", "wxa", "wxb", "wd0", "wd1", "wd2", "wd3"):
        names += [(kind, i) for i in range(8)]
    names += [(kind,) for kind in ("dyl", "dyr", "dya", "dyb", "dz7a", "dz7b")]
    names += [("dz", s) for s in range(1, 7)] + [("dd", i) for i in range(8)]
    names += [("s", j) for j in range(1, 4)]
    names += [("o", p) for p in range(1, 4)] + [("st", p) for p in range(1, 4)]
    names += [("a", j) for j in range(1, 4)]
    names += [(kind, h) for kind in ("fa", "fb", "u1", "u3", "m1", "m3") for h in range(2)]
    return names


NAMES = message_names()
INDEX = {name: i for i, name in enumerate(NAMES)}


def kernel(
    q1_ref, q2_ref, k1_ref, k2_ref, v_ref, g_ref, u_ref, d_ref, s_ref, lam_ref, hg_ref, ng_ref, wo_ref,
    out_ref,
    q_all, k_all, v_all, v_own, acc, m_st, l_st, sb0, sb1, w_all, d_all, s_all, wo_v,
    o_out, st_out, o_in, st_in, att, branch, row_sums, normed, hidden, part, part_in, far_in, merged_out,
    send_sems, recv_sems, local_sems,
):
    sp = lax.axis_index("sp")
    x = lax.axis_index("tp")
    z = sp // 8
    y = lax.rem(sp, 8) // 2
    c = lax.rem(sp, 2)

    def mod(a, n):
        return lax.rem(a + 2 * n, n)

    def at(dz=0, dy=0, dc=0, dx=0):
        return {
            "sp": mod(z + dz, 8) * 8 + mod(y + dy, 4) * 2 + mod(c + dc, 2),
            "tp": mod(x + dx, 4),
        }

    def block(dz=0, dy=0):
        return mod(z + dz, 8) * 8 + mod(y + dy, 4) * 2 + c

    def partial_rows(j, offset):
        return pl.ds(pl.multiple_of(mod(x - j, 4) * 64 + offset, 32), 32)

    def remote(name, src, dst, target):
        i = INDEX[name]
        return pltpu.make_async_remote_copy(
            src_ref=src, dst_ref=dst, send_sem=send_sems.at[i], recv_sem=recv_sems.at[i],
            device_id=target, device_id_type=MESH,
        )

    def describe(name):
        kind = name[0]
        if kind == "q":
            p = name[1]
            return remote(name, q_all.at[0], q_all.at[p], at(dy=REL[p]))
        if kind in ("k", "v"):
            s = name[1]
            buf = k_all if kind == "k" else v_all
            step = 1 if s in (1, 3, 5) else -1
            before = s - 2
            if s == 7:
                step, before = (1, 5) if kind == "k" else (-1, 6)
            return remote(name, buf.at[2 * max(before, 0)], buf.at[2 * s], at(dz=step))
        if kind in ("kd", "vd"):
            s = name[1]
            buf = k_all if kind == "kd" else v_all
            return remote(name, buf.at[2 * s], buf.at[2 * s + 1], at(dc=1))
        if kind == "wz":
            s = name[1]
            step = 1 if s in (1, 3, 5) else -1
            ref = w_all.at[block(dz=Z_OF_SLOT[s - 2] if s > 2 else 0)]
            return remote(name, ref, ref, at(dz=step))
        if kind == "wz7a":
            ref = w_all.at[block(dz=-3), 0:32]
            return remote(name, ref, ref, at(dz=1))
        if kind == "wz7b":
            ref = w_all.at[block(dz=3), 32:64]
            return remote(name, ref, ref, at(dz=-1))
        if kind in ("wxl", "wxr"):
            ref = w_all.at[block(dz=Z_OF_SLOT[name[1]])]
            return remote(name, ref, ref, at(dy=1 if kind == "wxl" else -1))
        if kind == "wxa":
            ref = w_all.at[block(dz=Z_OF_SLOT[name[1]], dy=-1), 0:32]
            return remote(name, ref, ref, at(dy=1))
        if kind == "wxb":
            ref = w_all.at[block(dz=Z_OF_SLOT[name[1]], dy=1), 32:64]
            return remote(name, ref, ref, at(dy=-1))
        if kind[:2] == "wd":
            ref = w_all.at[block(dz=Z_OF_SLOT[name[1]], dy=(0, -1, 1, 2)[int(kind[2])])]
            return remote(name, ref, ref, at(dc=1))
        if kind in ("dyl", "dyr"):
            ref = d_all.at[z, c, y]
            return remote(name, ref, ref, at(dy=1 if kind == "dyl" else -1))
        if kind == "dya":
            ref = d_all.at[z, c, mod(y - 1, 4), 0:16]
            return remote(name, ref, ref, at(dy=1))
        if kind == "dyb":
            ref = d_all.at[z, c, mod(y + 1, 4), 16:32]
            return remote(name, ref, ref, at(dy=-1))
        if kind == "dz":
            s = name[1]
            ref = d_all.at[mod(z + (Z_OF_SLOT[s - 2] if s > 2 else 0), 8), c]
            return remote(name, ref, ref, at(dz=1 if s in (1, 3, 5) else -1))
        if kind == "dz7a":
            ref = d_all.at[mod(z - 3, 8), c, 0:2]
            return remote(name, ref, ref, at(dz=1))
        if kind == "dz7b":
            ref = d_all.at[mod(z + 3, 8), c, 2:4]
            return remote(name, ref, ref, at(dz=-1))
        if kind == "dd":
            ref = d_all.at[mod(z + Z_OF_SLOT[name[1]], 8), c]
            return remote(name, ref, ref, at(dc=1))
        if kind == "s":
            return remote(name, s_all.at[x], s_all.at[x], at(dx=name[1]))
        if kind == "o":
            p = name[1]
            return remote(name, o_out.at[p - 1], o_in.at[p - 1], at(dy=-REL[p]))
        if kind == "st":
            p = name[1]
            return remote(name, st_out.at[p - 1], st_in.at[p - 1], at(dy=-REL[p]))
        if kind == "a":
            return remote(name, att.at[x], att.at[x], at(dx=name[1]))
        h = name[1]
        if kind == "fa":
            return remote(name, part.at[h, partial_rows(2, 0)], far_in.at[h, 0], at(dx=-1))
        if kind == "fb":
            return remote(name, part.at[h, partial_rows(2, 32)], far_in.at[h, 1], at(dx=1))
        if kind == "u1":
            return remote(name, part.at[h, partial_rows(1, 32)], part_in.at[h, 0, 32:64], at(dx=-1))
        if kind == "u3":
            return remote(name, part.at[h, partial_rows(3, 0)], part_in.at[h, 1, 0:32], at(dx=1))
        if kind == "m1":
            return remote(name, merged_out.at[h, 0], part_in.at[h, 0, 0:32], at(dx=-1))
        if kind == "m3":
            return remote(name, merged_out.at[h, 1], part_in.at[h, 1, 32:64], at(dx=1))
        raise KeyError(kind)

    def start(*names):
        for name in names:
            describe(name).start()

    def arrive(*names):
        for name in names:
            describe(name).wait_recv()

    barrier = pltpu.get_barrier_semaphore()
    partners = [at(dz=1), at(dz=-1), at(dc=1)]
    partners += [at(dy=j) for j in range(1, 4)] + [at(dx=j) for j in range(1, 4)]
    for partner in partners:
        pl.semaphore_signal(barrier, inc=1, device_id=partner, device_id_type=MESH)
    takes = [
        pltpu.make_async_copy(src, dst, local_sems.at[3 + i])
        for i, (src, dst) in enumerate((
            (v_ref, v_own), (q1_ref, q_all.at[0, :, 0:128]), (q2_ref, q_all.at[0, :, 128:256]),
            (k1_ref, k_all.at[0, :, 0:128]), (k2_ref, k_all.at[0, :, 128:256]),
            (g_ref, w_all.at[sp, 0:32]), (u_ref, w_all.at[sp, 32:64]), (d_ref, d_all.at[z, c, y]), (s_ref, s_all.at[x]),
        ))
    ]
    for take in takes:
        take.start()
    wo_copy = pltpu.make_async_copy(wo_ref, wo_v, local_sems.at[0])
    wo_copy.start()
    takes[0].wait()
    v_all[0] = jnp.transpose(v_own[...])
    for take in takes[1:]:
        take.wait()
    pl.semaphore_wait(barrier, len(partners))

    start(("q", 1), ("q", 2), ("kd", 0), ("k", 1), ("k", 2), ("vd", 0), ("v", 1), ("v", 2), ("q", 3))
    m_st[...] = jnp.full_like(m_st, -1e30)
    l_st[...] = jnp.zeros_like(l_st)
    acc[...] = jnp.zeros_like(acc)

    def w_across(i):
        def act():
            start(("wxl", i), ("wxr", i), ("wd0", i))
        return act

    def w_on(i):
        def act():
            arrive(("wxl", i), ("wxr", i))
            start(("wxa", i), ("wxb", i), ("wd1", i), ("wd2", i))
        return act

    def w_last(i):
        def act():
            arrive(("wxa", i), ("wxb", i))
            start(("wd3", i))
        return act

    def on(a, s):
        def act():
            arrive((a, s), (a, s + 1))
            if s < 5:
                start((a, s + 2), (a, s + 3))
            else:
                start((a, 7))
            start((a + "d", s), (a + "d", s + 1))
        return act

    def ring_end():
        arrive(("k", 7), ("v", 7))
        start(("kd", 7), ("vd", 7))

    def got(*names):
        return lambda: arrive(*names)

    def w_ring(s):
        def act():
            arrive(("wz", s), ("wz", s + 1))
            w_across(s)()
            w_across(s + 1)()
        return act

    def w_next(s):
        def act():
            if s < 5:
                start(("wz", s + 2), ("wz", s + 3))
            else:
                start(("wz7a",), ("wz7b",))
        return act

    def w_ring_end():
        arrive(("wz7a",), ("wz7b",))

    def finalize(p):
        def act():
            for hm in range(4):
                unit = p * 4 + hm
                total = jnp.sum(l_st[unit], axis=0, keepdims=True)
                o_out[p - 1, hm * 128:(hm + 1) * 128, :] = (acc[unit] * (1.0 / total)).astype(BF16)
                st_out[p - 1, hm:hm + 1, :] = m_st[unit, 0:1, :]
                st_out[p - 1, 4 + hm:5 + hm, :] = total
            start(("o", p), ("st", p))
        return act

    def d_first():
        start(("dyl",), ("dyr",))

    def d_on():
        arrive(("dyl",), ("dyr",))
        start(("dya",), ("dyb",))

    def d_last():
        arrive(("dya",), ("dyb",))
        start(("dd", 0))

    def d_ring(s):
        def act():
            arrive(("dz", s), ("dz", s + 1))
            if s < 5:
                start(("dz", s + 2), ("dz", s + 3))
            else:
                start(("dz7a",), ("dz7b",))
            start(("dd", s), ("dd", s + 1))
        return act

    phases = (
        (0, 2, (
            (got(("kd", 0), ("vd", 0)),),
            (got(("q", 2)), on("k", 1), lambda: start(("wz", 1), ("wz", 2)), w_across(0), d_first),
            (got(("q", 3)), on("v", 1)),
            (got(("kd", 1), ("kd", 2)),),
        )),
        (2, 4, (
            (got(("vd", 1), ("vd", 2)), lambda: start(("s", 1), ("s", 3), ("s", 2))),
            (on("k", 3), w_on(0), d_on),
            (w_ring(1), w_next(1)),
            (on("v", 3), got(("kd", 3), ("kd", 4))),
        )),
        (6, 4, (
            (got(("vd", 3), ("vd", 4)),),
            (w_last(0), d_last),
            (on("k", 5),),
            (got(("kd", 5), ("kd", 6)), w_on(1), on("v", 5)),
        )),
        (10, 4, (
            (w_ring(3), w_next(3), lambda: start(("dz", 1), ("dz", 2)), got(("vd", 5), ("vd", 6))),
            (w_on(2),),
            (w_last(1),),
            (ring_end, got(("kd", 7))),
        )),
        (14, 2, (
            (got(("vd", 7)), w_on(3)),
            (finalize(3), w_on(4), w_last(2)),
            (finalize(2),),
            (finalize(1), got(("wz", 5), ("wz", 6)), w_next(5)),
        )),
    )

    def scores(s_buf, qi, hm, first, count):
        m, h = hm // 2, hm % 2
        q = q_all[qi, :, m * 128:(m + 1) * 128]
        lane = lax.broadcasted_iota(jnp.int32, q.shape, 1)
        q = jnp.where((lane >= 64) if h else (lane < 64), q, jnp.zeros_like(q))
        peak = None
        for b in range(count):
            s = lax.dot_general(
                k_all[first + b, :, m * 128:(m + 1) * 128], q, (((1,), (1,)), ((), ())),
                preferred_element_type=F32,
            )
            s_buf[b * 256:(b + 1) * 256, :] = s
            r = jnp.max(s.reshape(32, 8, 256), axis=0)
            peak = r if peak is None else jnp.maximum(peak, r)
        return peak

    def absorb(s_buf, unit, hm, first, count, peak):
        h = hm % 2
        m_old = m_st[unit]
        m_new = jnp.maximum(m_old, jnp.max(peak, axis=0, keepdims=True) * SCALE)
        rescale = jnp.exp2(m_old - m_new)
        m_st[unit] = m_new
        total, out = None, None
        for b in range(count):
            s = s_buf[b * 256:(b + 1) * 256, :].reshape(32, 8, 256)
            weights = jnp.exp2(s * SCALE - m_new[None])
            t = jnp.sum(weights, axis=0)
            total = t if total is None else total + t
            o = jnp.dot(
                v_all[first + b, h * 128:(h + 1) * 128, :], weights.reshape(256, 256).astype(BF16),
                preferred_element_type=F32,
            )
            out = o if out is None else out + o
        l_st[unit] = l_st[unit] * rescale + total
        acc[unit] = (acc[unit].reshape(16, 8, 256) * rescale[None] + out.reshape(16, 8, 256)).reshape(128, 256)

    bufs = (sb0, sb1)

    def visit(qi, first, count, peak, qi_ahead, first_ahead, count_ahead):
        for hm in range(4):
            if hm < 3:
                ahead = scores(bufs[(hm + 1) % 2], qi, hm + 1, first, count)
            else:
                ahead = scores(bufs[0], qi_ahead, 0, first_ahead, count_ahead)
            absorb(bufs[hm % 2], qi * 4 + hm, hm, first, count, peak)
            peak = ahead
        return peak

    peak = None
    for n, (first, count, actions) in enumerate(phases):
        closing = n == len(phases) - 1
        for action in actions[0]:
            action()
        if peak is None:
            peak = scores(bufs[0], 0, 0, first, count)
            visit(0, first, count, peak, 0, first, count)
            arrive(("q", 1))
            peak = scores(bufs[0], 1, 0, first, count)

        def body(i, peak):
            for at_step in (1, 2):
                if actions[at_step]:
                    @pl.when(i == at_step)
                    def _():
                        for action in actions[at_step]:
                            action()
            qi = 3 - i if closing else i
            return visit(qi, first, count, peak, qi - 1 if closing else qi + 1, first, count)

        peak = lax.fori_loop(0 if n else 1, 3, body, peak)
        for action in actions[3]:
            action()
        if closing:
            visit(0, first, count, peak, 0, first, count)
        else:
            ahead = phases[n + 1]
            opening = 3 if n + 2 == len(phases) else 0
            peak = visit(3, first, count, peak, opening, ahead[0], ahead[1])

    w_last(3)()
    d_ring(1)()
    arrive(("o", 3), ("st", 3))
    w_across(5)()
    w_across(6)()
    w_ring_end()
    d_ring(3)()
    arrive(("o", 2), ("st", 2))
    arrive(("o", 1), ("st", 1))
    w_across(7)()
    for h in range(2):
        maps = []
        for m in range(2):
            hm = m * 2 + h
            unit = hm
            peaks = [st_in[p, hm:hm + 1, :] for p in range(3)] + [m_st[unit, 0:1, :]]
            sums = [st_in[p, 4 + hm:5 + hm, :] for p in range(3)] + [jnp.sum(l_st[unit], axis=0, keepdims=True)]
            top = functools.reduce(jnp.maximum, peaks)
            powers = [jnp.exp2(v - top) for v in peaks]
            total = sum(v * l for v, l in zip(powers, sums))
            inverse = 1.0 / total
            merged = acc[unit] * (powers[3] * inverse)
            for p in range(3):
                merged += o_in[p, hm * 128:(hm + 1) * 128, :].astype(F32) * (powers[p] * sums[p] * inverse)
            maps.append(merged)
        differ = maps[0] - lam_ref[h] * maps[1]
        mean_square = jnp.mean(differ * differ, axis=0, keepdims=True)
        scaled = jnp.transpose(differ * lax.rsqrt(mean_square + EPSILON))
        att[x, :, h * 128:(h + 1) * 128] = (scaled * hg_ref[...] * 0.8).astype(BF16)
    exchange = [("a", 2), ("a", 1), ("a", 3)]
    start(*exchange)
    w_last(4)()
    d_ring(5)()
    w_on(5)()
    w_on(6)()
    w_on(7)()
    wo_copy.wait()
    arrive(*exchange)

    arrive(("s", 1), ("s", 2), ("s", 3))
    row_sums[...] = jnp.zeros_like(row_sums)

    def project(n, carry):
        cols = pl.ds(pl.multiple_of(n * 512, 512), 512)
        total = None
        for i in range(4):
            term = jnp.dot(att[i], wo_v[i * 256:(i + 1) * 256, cols], preferred_element_type=F32)
            total = term if total is None else total + term
        mixed = ALPHA * s_all[:, :, cols].reshape(256, 512).astype(F32) + total
        branch[:, cols] = mixed
        row_sums[...] += sum(mixed[:, i * 128:(i + 1) * 128] for i in range(4))
        return carry

    lax.fori_loop(0, 4, project, 0)
    w_last(5)()
    w_last(6)()
    arrive(("dz7a",), ("dz7b",))
    start(("dd", 7))
    mean = jnp.sum(row_sums[...], axis=-1, keepdims=True) * (1.0 / 2048)
    row_sums[...] = jnp.broadcast_to(mean, (256, 128))
    spread = None
    for n in range(16):
        centered = branch[:, n * 128:(n + 1) * 128] - row_sums[...]
        spread = centered * centered if spread is None else spread + centered * centered
    var = jnp.sum(spread, axis=-1, keepdims=True) * (1.0 / 2048)
    inverse = jnp.broadcast_to(lax.rsqrt(var + EPSILON), (256, 128))
    for n in range(16):
        cols = slice(n * 128, (n + 1) * 128)
        normed[:, cols] = ((branch[:, cols] - row_sums[...]) * inverse * ng_ref[:, cols]).astype(BF16)
    w_last(7)()
    for kind in ("wd0", "wd1", "wd2", "wd3"):
        arrive(*[(kind, i) for i in range(8)])
    for lo, hi in ((0, 256), (256, 512), (512, 704)):
        gate = jnp.dot(normed[...], w_all[:, 0:32, lo:hi].reshape(2048, hi - lo), preferred_element_type=F32)
        upward = jnp.dot(normed[...], w_all[:, 32:64, lo:hi].reshape(2048, hi - lo), preferred_element_type=F32)
        hidden[:, lo:hi] = (gate / (1.0 + jnp.exp(-gate)) * upward).astype(BF16)
    arrive(*[("dd", i) for i in range(8)])
    for h in range(2):
        def down(n, carry):
            columns = jnp.concatenate([d_all[h * 4 + n, i % 2, i // 2] for i in range(8)], axis=0)
            product = lax.dot_general(
                hidden[...], columns, (((1,), (1,)), ((), ())),
                preferred_element_type=F32,
            ).astype(BF16)
            cols = pl.ds(pl.multiple_of(n * 256, 256), 256)
            part[h, :, cols] = product
            return carry

        lax.fori_loop(0, 4, down, 0)
        start(("fa", h), ("fb", h), ("u1", h), ("u3", h))
    for h in range(2):
        arrive(("fa", h), ("fb", h))
        for side, (j, offset) in enumerate(((1, 0), (3, 32))):
            own = part[h, partial_rows(j, offset), :].astype(F32)
            merged_out[h, side] = (own + far_in[h, side].astype(F32)).astype(BF16)
        start(("m1", h), ("m3", h))
    own_rows = pl.ds(pl.multiple_of(x * 64, 64), 64)
    for h in range(2):
        arrive(("u1", h), ("u3", h), ("m1", h), ("m3", h))
        cols = slice(h * 1024, (h + 1) * 1024)
        mixer = part[h, own_rows, :].astype(F32)
        for side in range(2):
            mixer += part_in[h, side].astype(F32)
        out_ref[:, cols] = (ALPHA * normed[own_rows, cols].astype(F32) + 0.5 * mixer).astype(BF16)
    for name in NAMES:
        describe(name).wait_send()


def on_device(
    stream, query_one, key_one, query_two, key_two, values, lambdas, head_gain, out_weight, norm_gain,
    gate_weight, up_weight, down_weight,
):
    whole = pl.BlockSpec(memory_space=pl.ANY)
    vmem = pl.BlockSpec(memory_space=pltpu.VMEM)
    return pl.pallas_call(
        kernel,
        out_shape=jax.ShapeDtypeStruct((64, 2048), BF16),
        in_specs=[whole] * 9 + [pl.BlockSpec(memory_space=pltpu.SMEM), vmem, vmem, whole],
        out_specs=vmem,
        scratch_shapes=[
            pltpu.VMEM((4, 256, 256), BF16),
            pltpu.VMEM((16, 256, 256), BF16),
            pltpu.VMEM((16, 256, 256), BF16),
            pltpu.VMEM((256, 256), BF16),
            pltpu.VMEM((16, 128, 256), F32),
            pltpu.VMEM((16, 8, 256), F32),
            pltpu.VMEM((16, 8, 256), F32),
            pltpu.VMEM((1024, 256), F32),
            pltpu.VMEM((1024, 256), F32),
            pltpu.VMEM((64, 64, 704), BF16),
            pltpu.VMEM((8, 2, 4, 32, 704), BF16),
            pltpu.VMEM((4, 64, 2048), BF16),
            pltpu.VMEM((1024, 2048), BF16),
            pltpu.VMEM((3, 512, 256), BF16),
            pltpu.VMEM((3, 8, 256), F32),
            pltpu.VMEM((3, 512, 256), BF16),
            pltpu.VMEM((3, 8, 256), F32),
            pltpu.VMEM((4, 256, 256), BF16),
            pltpu.VMEM((256, 2048), F32),
            pltpu.VMEM((256, 128), F32),
            pltpu.VMEM((256, 2048), BF16),
            pltpu.VMEM((256, 704), BF16),
            pltpu.VMEM((2, 256, 1024), BF16),
            pltpu.VMEM((2, 2, 64, 1024), BF16),
            pltpu.VMEM((2, 2, 32, 1024), BF16),
            pltpu.VMEM((2, 2, 32, 1024), BF16),
            pltpu.SemaphoreType.DMA((len(NAMES),)),
            pltpu.SemaphoreType.DMA((len(NAMES),)),
            pltpu.SemaphoreType.DMA((12,)),
        ],
        compiler_params=pltpu.CompilerParams(
            collective_id=0, has_side_effects=True, vmem_limit_bytes=60 * 2**20
        ),
    )(
        query_one, query_two, key_one, key_two, values, gate_weight, up_weight, jnp.transpose(down_weight), stream, lambdas, head_gain.reshape(1, 128), norm_gain.reshape(1, 2048),
        out_weight,
    )


def solution(mesh):
    return jax.shard_map(
        on_device,
        mesh=mesh,
        in_specs=(
            P(("sp", "tp"), None), P("sp", "tp"), P("sp", "tp"), P("sp", "tp"), P("sp", "tp"), P("sp", "tp"),
            P("tp"), P(), P(), P(), P("sp", "tp"), P("sp", "tp"), P("tp", "sp"),
        ),
        out_specs=P(("sp", "tp"), None),
        check_vma=False,
    )
```

```python
import functools
import math

import jax
import jax.numpy as jnp
from jax import lax
from jax.experimental import pallas as pl
from jax.experimental.pallas import tpu as pltpu
from jax.sharding import PartitionSpec as P

MESH = pl.DeviceIdType.MESH
F32 = jnp.float32
BF16 = jnp.bfloat16
ALPHA = 1.4142135623730951
EPSILON = 1e-05
SCALE = math.log2(math.e) / 8.0
REL = (0, 1, 3, 2)
Z_OF_SLOT = (0, -1, 1, -2, 2, -3, 3, 4)


def message_names():
    names = [("q", p) for p in range(1, 4)]
    for a in "kv":
        names += [(a, s) for s in range(1, 8)] + [(a + "d", s) for s in range(8)]
    names += [("wz", s) for s in range(1, 7)] + [("wz7a",), ("wz7b",)]
    for kind in ("wxl", "wxr", "wxa", "wxb", "wd0", "wd1", "wd2", "wd3"):
        names += [(kind, i) for i in range(8)]
    names += [(kind,) for kind in ("dyl", "dyr", "dya", "dyb", "dz7a", "dz7b")]
    names += [("dz", s) for s in range(1, 7)] + [("dd", i) for i in range(8)]
    names += [("s", j) for j in range(1, 4)]
    names += [("o", p) for p in range(1, 4)] + [("st", p) for p in range(1, 4)]
    names += [("a", j) for j in range(1, 4)]
    names += [(kind, h) for kind in ("fa", "fb", "u1", "u3", "m1", "m3") for h in range(2)]
    return names


NAMES = message_names()
INDEX = {name: i for i, name in enumerate(NAMES)}


def kernel(
    q1_ref, q2_ref, k1_ref, k2_ref, v_ref, g_ref, u_ref, d_ref, s_ref, lam_ref, hg_ref, ng_ref, wo_ref,
    out_ref,
    q_all, k_all, v_all, v_own, acc, m_st, l_st, sb0, sb1, w_all, d_all, s_all, wo_v,
    o_out, st_out, o_in, st_in, att, branch, row_sums, normed, hidden, part, part_in, far_in, merged_out,
    send_sems, recv_sems, local_sems,
):
    sp = lax.axis_index("sp")
    x = lax.axis_index("tp")
    z = sp // 8
    y = lax.rem(sp, 8) // 2
    c = lax.rem(sp, 2)

    def mod(a, n):
        return lax.rem(a + 2 * n, n)

    def at(dz=0, dy=0, dc=0, dx=0):
        return {
            "sp": mod(z + dz, 8) * 8 + mod(y + dy, 4) * 2 + mod(c + dc, 2),
            "tp": mod(x + dx, 4),
        }

    def block(dz=0, dy=0):
        return mod(z + dz, 8) * 8 + mod(y + dy, 4) * 2 + c

    def partial_rows(j, offset):
        return pl.ds(pl.multiple_of(mod(x - j, 4) * 64 + offset, 32), 32)

    def remote(name, src, dst, target):
        i = INDEX[name]
        return pltpu.make_async_remote_copy(
            src_ref=src, dst_ref=dst, send_sem=send_sems.at[i], recv_sem=recv_sems.at[i],
            device_id=target, device_id_type=MESH,
        )

    def describe(name):
        kind = name[0]
        if kind == "q":
            p = name[1]
            return remote(name, q_all.at[0], q_all.at[p], at(dy=REL[p]))
        if kind in ("k", "v"):
            s = name[1]
            buf = k_all if kind == "k" else v_all
            step = 1 if s in (1, 3, 5) else -1
            before = s - 2
            if s == 7:
                step, before = (1, 5) if kind == "k" else (-1, 6)
            return remote(name, buf.at[2 * max(before, 0)], buf.at[2 * s], at(dz=step))
        if kind in ("kd", "vd"):
            s = name[1]
            buf = k_all if kind == "kd" else v_all
            return remote(name, buf.at[2 * s], buf.at[2 * s + 1], at(dc=1))
        if kind == "wz":
            s = name[1]
            step = 1 if s in (1, 3, 5) else -1
            ref = w_all.at[block(dz=Z_OF_SLOT[s - 2] if s > 2 else 0)]
            return remote(name, ref, ref, at(dz=step))
        if kind == "wz7a":
            ref = w_all.at[block(dz=-3), 0:32]
            return remote(name, ref, ref, at(dz=1))
        if kind == "wz7b":
            ref = w_all.at[block(dz=3), 32:64]
            return remote(name, ref, ref, at(dz=-1))
        if kind in ("wxl", "wxr"):
            ref = w_all.at[block(dz=Z_OF_SLOT[name[1]])]
            return remote(name, ref, ref, at(dy=1 if kind == "wxl" else -1))
        if kind == "wxa":
            ref = w_all.at[block(dz=Z_OF_SLOT[name[1]], dy=-1), 0:32]
            return remote(name, ref, ref, at(dy=1))
        if kind == "wxb":
            ref = w_all.at[block(dz=Z_OF_SLOT[name[1]], dy=1), 32:64]
            return remote(name, ref, ref, at(dy=-1))
        if kind[:2] == "wd":
            ref = w_all.at[block(dz=Z_OF_SLOT[name[1]], dy=(0, -1, 1, 2)[int(kind[2])])]
            return remote(name, ref, ref, at(dc=1))
        if kind in ("dyl", "dyr"):
            ref = d_all.at[z, c, y]
            return remote(name, ref, ref, at(dy=1 if kind == "dyl" else -1))
        if kind == "dya":
            ref = d_all.at[z, c, mod(y - 1, 4), 0:16]
            return remote(name, ref, ref, at(dy=1))
        if kind == "dyb":
            ref = d_all.at[z, c, mod(y + 1, 4), 16:32]
            return remote(name, ref, ref, at(dy=-1))
        if kind == "dz":
            s = name[1]
            ref = d_all.at[mod(z + (Z_OF_SLOT[s - 2] if s > 2 else 0), 8), c]
            return remote(name, ref, ref, at(dz=1 if s in (1, 3, 5) else -1))
        if kind == "dz7a":
            ref = d_all.at[mod(z - 3, 8), c, 0:2]
            return remote(name, ref, ref, at(dz=1))
        if kind == "dz7b":
            ref = d_all.at[mod(z + 3, 8), c, 2:4]
            return remote(name, ref, ref, at(dz=-1))
        if kind == "dd":
            ref = d_all.at[mod(z + Z_OF_SLOT[name[1]], 8), c]
            return remote(name, ref, ref, at(dc=1))
        if kind == "s":
            return remote(name, s_all.at[x], s_all.at[x], at(dx=name[1]))
        if kind == "o":
            p = name[1]
            return remote(name, o_out.at[p - 1], o_in.at[p - 1], at(dy=-REL[p]))
        if kind == "st":
            p = name[1]
            return remote(name, st_out.at[p - 1], st_in.at[p - 1], at(dy=-REL[p]))
        if kind == "a":
            return remote(name, att.at[x], att.at[x], at(dx=name[1]))
        h = name[1]
        if kind == "fa":
            return remote(name, part.at[h, partial_rows(2, 0)], far_in.at[h, 0], at(dx=-1))
        if kind == "fb":
            return remote(name, part.at[h, partial_rows(2, 32)], far_in.at[h, 1], at(dx=1))
        if kind == "u1":
            return remote(name, part.at[h, partial_rows(1, 32)], part_in.at[h, 0, 32:64], at(dx=-1))
        if kind == "u3":
            return remote(name, part.at[h, partial_rows(3, 0)], part_in.at[h, 1, 0:32], at(dx=1))
        if kind == "m1":
            return remote(name, merged_out.at[h, 0], part_in.at[h, 0, 0:32], at(dx=-1))
        if kind == "m3":
            return remote(name, merged_out.at[h, 1], part_in.at[h, 1, 32:64], at(dx=1))
        raise KeyError(kind)

    def start(*names):
        for name in names:
            describe(name).start()

    def arrive(*names):
        for name in names:
            describe(name).wait_recv()

    barrier = pltpu.get_barrier_semaphore()
    partners = [at(dz=1), at(dz=-1), at(dc=1)]
    partners += [at(dy=j) for j in range(1, 4)] + [at(dx=j) for j in range(1, 4)]
    for partner in partners:
        pl.semaphore_signal(barrier, inc=1, device_id=partner, device_id_type=MESH)
    takes = [
        pltpu.make_async_copy(src, dst, local_sems.at[3 + i])
        for i, (src, dst) in enumerate((
            (v_ref, v_own), (q1_ref, q_all.at[0, :, 0:128]), (q2_ref, q_all.at[0, :, 128:256]),
            (k1_ref, k_all.at[0, :, 0:128]), (k2_ref, k_all.at[0, :, 128:256]),
            (g_ref, w_all.at[sp, 0:32]), (u_ref, w_all.at[sp, 32:64]), (d_ref, d_all.at[z, c, y]), (s_ref, s_all.at[x]),
        ))
    ]
    for take in takes:
        take.start()
    wo_copy = pltpu.make_async_copy(wo_ref, wo_v, local_sems.at[0])
    wo_copy.start()
    takes[0].wait()
    v_all[0] = jnp.transpose(v_own[...])
    for take in takes[1:]:
        take.wait()
    pl.semaphore_wait(barrier, len(partners))

    start(("q", 1), ("q", 2), ("kd", 0), ("k", 1), ("k", 2), ("vd", 0), ("v", 1), ("v", 2), ("q", 3))
    m_st[...] = jnp.full_like(m_st, -1e30)
    l_st[...] = jnp.zeros_like(l_st)
    acc[...] = jnp.zeros_like(acc)

    def w_across(i):
        def act():
            start(("wxl", i), ("wxr", i), ("wd0", i))
        return act

    def w_on(i):
        def act():
            arrive(("wxl", i), ("wxr", i))
            start(("wxa", i), ("wxb", i), ("wd1", i), ("wd2", i))
        return act

    def w_last(i):
        def act():
            arrive(("wxa", i), ("wxb", i))
            start(("wd3", i))
        return act

    def on(a, s):
        def act():
            arrive((a, s), (a, s + 1))
            if s < 5:
                start((a, s + 2), (a, s + 3))
            else:
                start((a, 7))
            start((a + "d", s), (a + "d", s + 1))
        return act

    def ring_end():
        arrive(("k", 7), ("v", 7))
        start(("kd", 7), ("vd", 7))

    def got(*names):
        return lambda: arrive(*names)

    def w_ring(s):
        def act():
            arrive(("wz", s), ("wz", s + 1))
            w_across(s)()
            w_across(s + 1)()
        return act

    def w_next(s):
        def act():
            if s < 5:
                start(("wz", s + 2), ("wz", s + 3))
            else:
                start(("wz7a",), ("wz7b",))
        return act

    def w_ring_end():
        arrive(("wz7a",), ("wz7b",))

    def finalize(p):
        def act():
            for hm in range(4):
                unit = p * 4 + hm
                total = jnp.sum(l_st[unit], axis=0, keepdims=True)
                o_out[p - 1, hm * 128:(hm + 1) * 128, :] = (acc[unit] * (1.0 / total)).astype(BF16)
                st_out[p - 1, hm:hm + 1, :] = m_st[unit, 0:1, :]
                st_out[p - 1, 4 + hm:5 + hm, :] = total
            start(("o", p), ("st", p))
        return act

    def d_first():
        start(("dyl",), ("dyr",))

    def d_on():
        arrive(("dyl",), ("dyr",))
        start(("dya",), ("dyb",))

    def d_last():
        arrive(("dya",), ("dyb",))
        start(("dd", 0))

    def d_ring(s):
        def act():
            arrive(("dz", s), ("dz", s + 1))
            if s < 5:
                start(("dz", s + 2), ("dz", s + 3))
            else:
                start(("dz7a",), ("dz7b",))
            start(("dd", s), ("dd", s + 1))
        return act

    phases = (
        (0, 2, (
            (got(("kd", 0), ("vd", 0)),),
            (got(("q", 2)), on("k", 1), lambda: start(("wz", 1), ("wz", 2)), w_across(0), d_first),
            (got(("q", 3)), on("v", 1)),
            (got(("kd", 1), ("kd", 2)),),
        )),
        (2, 4, (
            (got(("vd", 1), ("vd", 2)), lambda: start(("s", 1), ("s", 3), ("s", 2))),
            (on("k", 3), w_on(0), d_on),
            (w_ring(1), w_next(1)),
            (on("v", 3), got(("kd", 3), ("kd", 4))),
        )),
        (6, 4, (
            (got(("vd", 3), ("vd", 4)),),
            (w_last(0), d_last),
            (on("k", 5),),
            (got(("kd", 5), ("kd", 6)), w_on(1), on("v", 5)),
        )),
        (10, 4, (
            (w_ring(3), w_next(3), lambda: start(("dz", 1), ("dz", 2)), got(("vd", 5), ("vd", 6))),
            (w_on(2),),
            (w_last(1),),
            (ring_end, got(("kd", 7))),
        )),
        (14, 2, (
            (got(("vd", 7)), w_on(3)),
            (finalize(3), w_on(4), w_last(2)),
            (finalize(2),),
            (finalize(1), got(("wz", 5), ("wz", 6)), w_next(5)),
        )),
    )

    def scores(s_buf, qi, hm, first, count):
        m, h = hm // 2, hm % 2
        q = q_all[qi, :, m * 128:(m + 1) * 128]
        lane = lax.broadcasted_iota(jnp.int32, q.shape, 1)
        q = jnp.where((lane >= 64) if h else (lane < 64), q, jnp.zeros_like(q))
        peak = None
        for b in range(count):
            s = lax.dot_general(
                k_all[first + b, :, m * 128:(m + 1) * 128], q, (((1,), (1,)), ((), ())),
                preferred_element_type=F32,
            )
            s_buf[b * 256:(b + 1) * 256, :] = s
            r = jnp.max(s.reshape(32, 8, 256), axis=0)
            peak = r if peak is None else jnp.maximum(peak, r)
        return peak

    def absorb(s_buf, unit, hm, first, count, peak):
        h = hm % 2
        m_old = m_st[unit]
        m_new = jnp.maximum(m_old, jnp.max(peak, axis=0, keepdims=True) * SCALE)
        rescale = jnp.exp2(m_old - m_new)
        m_st[unit] = m_new
        total, out = None, None
        for b in range(count):
            s = s_buf[b * 256:(b + 1) * 256, :].reshape(32, 8, 256)
            weights = jnp.exp2(s * SCALE - m_new[None])
            t = jnp.sum(weights, axis=0)
            total = t if total is None else total + t
            o = jnp.dot(
                v_all[first + b, h * 128:(h + 1) * 128, :], weights.reshape(256, 256).astype(BF16),
                preferred_element_type=F32,
            )
            out = o if out is None else out + o
        l_st[unit] = l_st[unit] * rescale + total
        acc[unit] = (acc[unit].reshape(16, 8, 256) * rescale[None] + out.reshape(16, 8, 256)).reshape(128, 256)

    bufs = (sb0, sb1)

    def visit(qi, first, count, peak, qi_ahead, first_ahead, count_ahead):
        for hm in range(4):
            if hm < 3:
                ahead = scores(bufs[(hm + 1) % 2], qi, hm + 1, first, count)
            else:
                ahead = scores(bufs[0], qi_ahead, 0, first_ahead, count_ahead)
            absorb(bufs[hm % 2], qi * 4 + hm, hm, first, count, peak)
            peak = ahead
        return peak

    peak = None
    for n, (first, count, actions) in enumerate(phases):
        closing = n == len(phases) - 1
        for action in actions[0]:
            action()
        if peak is None:
            peak = scores(bufs[0], 0, 0, first, count)
            visit(0, first, count, peak, 0, first, count)
            arrive(("q", 1))
            peak = scores(bufs[0], 1, 0, first, count)

        def body(i, peak):
            for at_step in (1, 2):
                if actions[at_step]:
                    @pl.when(i == at_step)
                    def _():
                        for action in actions[at_step]:
                            action()
            qi = 3 - i if closing else i
            return visit(qi, first, count, peak, qi - 1 if closing else qi + 1, first, count)

        peak = lax.fori_loop(0 if n else 1, 3, body, peak)
        for action in actions[3]:
            action()
        if closing:
            visit(0, first, count, peak, 0, first, count)
        else:
            ahead = phases[n + 1]
            opening = 3 if n + 2 == len(phases) else 0
            peak = visit(3, first, count, peak, opening, ahead[0], ahead[1])

    w_last(3)()
    d_ring(1)()
    arrive(("o", 3), ("st", 3))
    w_across(5)()
    w_across(6)()
    w_ring_end()
    d_ring(3)()
    arrive(("o", 2), ("st", 2))
    arrive(("o", 1), ("st", 1))
    w_across(7)()
    for h in range(2):
        maps = []
        for m in range(2):
            hm = m * 2 + h
            unit = hm
            peaks = [st_in[p, hm:hm + 1, :] for p in range(3)] + [m_st[unit, 0:1, :]]
            sums = [st_in[p, 4 + hm:5 + hm, :] for p in range(3)] + [jnp.sum(l_st[unit], axis=0, keepdims=True)]
            top = functools.reduce(jnp.maximum, peaks)
            powers = [jnp.exp2(v - top) for v in peaks]
            total = sum(v * l for v, l in zip(powers, sums))
            inverse = 1.0 / total
            merged = acc[unit] * (powers[3] * inverse)
            for p in range(3):
                merged += o_in[p, hm * 128:(hm + 1) * 128, :].astype(F32) * (powers[p] * sums[p] * inverse)
            maps.append(merged)
        differ = maps[0] - lam_ref[h] * maps[1]
        mean_square = jnp.mean(differ * differ, axis=0, keepdims=True)
        scaled = jnp.transpose(differ * lax.rsqrt(mean_square + EPSILON))
        att[x, :, h * 128:(h + 1) * 128] = (scaled * hg_ref[...] * 0.8).astype(BF16)
    exchange = [("a", 2), ("a", 1), ("a", 3)]
    start(*exchange)
    w_last(4)()
    d_ring(5)()
    w_on(5)()
    w_on(6)()
    w_on(7)()
    wo_copy.wait()
    arrive(*exchange)

    arrive(("s", 1), ("s", 2), ("s", 3))
    row_sums[...] = jnp.zeros_like(row_sums)

    def project(n, carry):
        cols = pl.ds(pl.multiple_of(n * 512, 512), 512)
        total = None
        for i in range(4):
            term = jnp.dot(att[i], wo_v[i * 256:(i + 1) * 256, cols], preferred_element_type=F32)
            total = term if total is None else total + term
        mixed = ALPHA * s_all[:, :, cols].reshape(256, 512).astype(F32) + total
        branch[:, cols] = mixed
        row_sums[...] += sum(mixed[:, i * 128:(i + 1) * 128] for i in range(4))
        return carry

    lax.fori_loop(0, 4, project, 0, unroll=True)
    w_last(5)()
    w_last(6)()
    arrive(("dz7a",), ("dz7b",))
    start(("dd", 7))
    mean = jnp.sum(row_sums[...], axis=-1, keepdims=True) * (1.0 / 2048)
    row_sums[...] = jnp.broadcast_to(mean, (256, 128))
    spread = None
    for n in range(16):
        centered = branch[:, n * 128:(n + 1) * 128] - row_sums[...]
        spread = centered * centered if spread is None else spread + centered * centered
    var = jnp.sum(spread, axis=-1, keepdims=True) * (1.0 / 2048)
    inverse = jnp.broadcast_to(lax.rsqrt(var + EPSILON), (256, 128))
    for n in range(16):
        cols = slice(n * 128, (n + 1) * 128)
        normed[:, cols] = ((branch[:, cols] - row_sums[...]) * inverse * ng_ref[:, cols]).astype(BF16)
    w_last(7)()
    for kind in ("wd0", "wd1", "wd2", "wd3"):
        arrive(*[(kind, i) for i in range(8)])
    for lo, hi in ((0, 256), (256, 512), (512, 704)):
        gate = jnp.dot(normed[...], w_all[:, 0:32, lo:hi].reshape(2048, hi - lo), preferred_element_type=F32)
        upward = jnp.dot(normed[...], w_all[:, 32:64, lo:hi].reshape(2048, hi - lo), preferred_element_type=F32)
        hidden[:, lo:hi] = (gate / (1.0 + jnp.exp(-gate)) * upward).astype(BF16)
    arrive(*[("dd", i) for i in range(8)])
    for h in range(2):
        def down(n, carry):
            columns = jnp.concatenate([d_all[h * 4 + n, i % 2, i // 2] for i in range(8)], axis=0)
            product = lax.dot_general(
                hidden[...], columns, (((1,), (1,)), ((), ())),
                preferred_element_type=F32,
            ).astype(BF16)
            cols = pl.ds(pl.multiple_of(n * 256, 256), 256)
            part[h, :, cols] = product
            return carry

        lax.fori_loop(0, 4, down, 0, unroll=True)
        start(("fa", h), ("fb", h), ("u1", h), ("u3", h))
    for h in range(2):
        arrive(("fa", h), ("fb", h))
        for side, (j, offset) in enumerate(((1, 0), (3, 32))):
            own = part[h, partial_rows(j, offset), :].astype(F32)
            merged_out[h, side] = (own + far_in[h, side].astype(F32)).astype(BF16)
        start(("m1", h), ("m3", h))
    own_rows = pl.ds(pl.multiple_of(x * 64, 64), 64)
    for h in range(2):
        arrive(("u1", h), ("u3", h), ("m1", h), ("m3", h))
        cols = slice(h * 1024, (h + 1) * 1024)
        mixer = part[h, own_rows, :].astype(F32)
        for side in range(2):
            mixer += part_in[h, side].astype(F32)
        out_ref[:, cols] = (ALPHA * normed[own_rows, cols].astype(F32) + 0.5 * mixer).astype(BF16)
    for name in NAMES:
        describe(name).wait_send()


def on_device(
    stream, query_one, key_one, query_two, key_two, values, lambdas, head_gain, out_weight, norm_gain,
    gate_weight, up_weight, down_weight,
):
    whole = pl.BlockSpec(memory_space=pl.ANY)
    vmem = pl.BlockSpec(memory_space=pltpu.VMEM)
    return pl.pallas_call(
        kernel,
        out_shape=jax.ShapeDtypeStruct((64, 2048), BF16),
        in_specs=[whole] * 9 + [pl.BlockSpec(memory_space=pltpu.SMEM), vmem, vmem, whole],
        out_specs=vmem,
        scratch_shapes=[
            pltpu.VMEM((4, 256, 256), BF16),
            pltpu.VMEM((16, 256, 256), BF16),
            pltpu.VMEM((16, 256, 256), BF16),
            pltpu.VMEM((256, 256), BF16),
            pltpu.VMEM((16, 128, 256), F32),
            pltpu.VMEM((16, 8, 256), F32),
            pltpu.VMEM((16, 8, 256), F32),
            pltpu.VMEM((1024, 256), F32),
            pltpu.VMEM((1024, 256), F32),
            pltpu.VMEM((64, 64, 704), BF16),
            pltpu.VMEM((8, 2, 4, 32, 704), BF16),
            pltpu.VMEM((4, 64, 2048), BF16),
            pltpu.VMEM((1024, 2048), BF16),
            pltpu.VMEM((3, 512, 256), BF16),
            pltpu.VMEM((3, 8, 256), F32),
            pltpu.VMEM((3, 512, 256), BF16),
            pltpu.VMEM((3, 8, 256), F32),
            pltpu.VMEM((4, 256, 256), BF16),
            pltpu.VMEM((256, 2048), F32),
            pltpu.VMEM((256, 128), F32),
            pltpu.VMEM((256, 2048), BF16),
            pltpu.VMEM((256, 704), BF16),
            pltpu.VMEM((2, 256, 1024), BF16),
            pltpu.VMEM((2, 2, 64, 1024), BF16),
            pltpu.VMEM((2, 2, 32, 1024), BF16),
            pltpu.VMEM((2, 2, 32, 1024), BF16),
            pltpu.SemaphoreType.DMA((len(NAMES),)),
            pltpu.SemaphoreType.DMA((len(NAMES),)),
            pltpu.SemaphoreType.DMA((12,)),
        ],
        compiler_params=pltpu.CompilerParams(
            collective_id=0, has_side_effects=True, vmem_limit_bytes=60 * 2**20
        ),
    )(
        query_one, query_two, key_one, key_two, values, gate_weight, up_weight, jnp.transpose(down_weight), stream, lambdas, head_gain.reshape(1, 128), norm_gain.reshape(1, 2048),
        out_weight,
    )


def solution(mesh):
    return jax.shard_map(
        on_device,
        mesh=mesh,
        in_specs=(
            P(("sp", "tp"), None), P("sp", "tp"), P("sp", "tp"), P("sp", "tp"), P("sp", "tp"), P("sp", "tp"),
            P("tp"), P(), P(), P(), P("sp", "tp"), P("sp", "tp"), P("tp", "sp"),
        ),
        out_specs=P(("sp", "tp"), None),
        check_vma=False,
    )
```
